32 devices in a mesh: ep: 8 (over z, y), tp: 4 (over x, core).
Axes of the slice: x: 2, y: 2, z: 4, core: 2. Of those that a mesh axis runs over, the one named last changes fastest.
Arguments:
- tokens: bfloat16 [192, 1024], P('ep'), may hold values from -1.796875 to 1.796875
- attn_gain: float32 [1024], replicated, may hold values from 0.1 to 1.9
- w_query: bfloat16 [1024, 1024], P(None, 'tp'), may hold values from -0.1875 to 0.1875
- w_key: bfloat16 [1024, 256], P(None, 'tp'), may hold values from -0.1875 to 0.1875
- w_value: bfloat16 [1024, 256], P(None, 'tp'), may hold values from -0.1875 to 0.1875
- w_forget: bfloat16 [1024, 4], P(None, 'tp'), may hold values from -0.1875 to 0.1875
- forget_bias: float32 [4], P('tp'), may hold values from -1 to 2
- query_gain: float32 [64], replicated, may hold values from 0.1 to 1.9
- key_gain: float32 [64], replicated, may hold values from 0.1 to 1.9
- cache_pairs: bfloat16 [192, 4, 1024, 128], P('ep', 'tp'), may hold values from -6 to 206
- cache_cum: float32 [192, 4, 1024], P('ep', 'tp'), may hold values from -1024 to 0, as said below
- lengths: int32 [192], P('ep'), may hold values from 64 to 1024, as said below
- w_output: bfloat16 [1024, 1024], P('tp'), may hold values from -0.1875 to 0.1875
- ffn_gain: float32 [1024], replicated, may hold values from 0.1 to 1.9
- expert_ids: int32 [192, 2], replicated, may hold values from 0 to 7, all different within a row; in each aligned block of 24 rows (0 to 23, 24 to 47, ...) at most 16 rows name the same one
- route_weight: float32 [192, 2], replicated, may hold values from 0.2 to 1
- w_exp_gate: bfloat16 [8, 1024, 3584], P('ep', None, 'tp'), may hold values from -0.1875 to 0.1875
- w_exp_up: bfloat16 [8, 1024, 3584], P('ep', None, 'tp'), may hold values from -0.1875 to 0.1875
- w_exp_down: bfloat16 [8, 3584, 1024], P('ep', 'tp'), may hold values from -0.09375 to 0.09375
- shared_gate: bfloat16 [1024], replicated, may hold values from -0.1875 to 0.1875
- w_dense_gate: bfloat16 [4096, 1024], P('ep'), may hold values from -0.1875 to 0.1875
- w_dense_up: bfloat16 [4096, 1024], P('ep'), may hold values from -0.1875 to 0.1875
- w_dense_down: bfloat16 [4096, 1024], P('ep', 'tp'), may hold values from -0.09375 to 0.09375
Outputs:
- layer_out: bfloat16 [192, 1024], P('ep', 'tp')
The draws below stay inside these ranges and needn't reach their ends.
Inputs may be any that keep to these rules, and one draw needn't show every extreme that they name: The cache of sequence b holds positions 0 to lengths[b] - 1; some sequence has 1024. `expert_ids`: each row names 2 different experts; in each aligned block of 24 rows no expert is named by more than 16 rows. cache_cum[b, g, s] never rises with s.
All inputs are finite; a program needn't handle non-finite values.
Results may differ from the reference program's by a relative error of at most 0.02.
Values may be sent and summed in bfloat16 or wider, within the bound.
A program may use at most 64 MiB of HBM per device.

```python
import math
import jax
import jax.numpy as jnp
import numpy as np
from jax import lax

D = 1024
HEADS = 16
HEAD_DIM = 64
KV_HEADS = 4
FF_EXPERT = 3584
DENSE_FF = 4096
TOP_K = 2
SEQ_GRP = 24
CACHE_SLOTS = 1024
BATCH = 192
EXPERTS = 8
CAP = 16
HEAD_GROUP = 4
N_EP = 8
N_TP = 4


def draw_lengths(key, part):
    lengths_drawn = jax.random.randint(key, (BATCH,), CACHE_SLOTS // 16, CACHE_SLOTS + 1, dtype=jnp.int32)
    return lengths_drawn.at[0].set(CACHE_SLOTS)


def draw_cache_pairs(key, part):
    base_key = jax.random.fold_in(key, 0)
    complete_shape = (BATCH, KV_HEADS, CACHE_SLOTS, 2 * HEAD_DIM)
    entries = jnp.clip(jax.random.normal(base_key, complete_shape, jnp.float32), -6.0, 6.0)
    return entries.astype(jnp.bfloat16)


def draw_cache_cum(key, part):
    key_sequence = jax.random.split(key, 8)
    complete_shape = (BATCH, KV_HEADS, CACHE_SLOTS)
    head_shape = (BATCH, KV_HEADS, 1)
    slow_share = 0.5
    sluggish_flag = jax.random.uniform(key_sequence[0], head_shape) < slow_share
    whole_rate = jnp.exp(jax.random.uniform(key_sequence[1], head_shape, jnp.float32, jnp.log(0.4), jnp.log(2.0))) / CACHE_SLOTS
    quick_rate = 1.0 / jax.random.uniform(key_sequence[2], head_shape, jnp.float32, 30.0, 50.0)
    step_frequency = jnp.where(sluggish_flag, whole_rate, quick_rate)
    device_multiplier = jnp.exp(jax.random.uniform(key_sequence[3], head_shape, jnp.float32, jnp.log(0.5), jnp.log(2.0)))
    block_multiplier = jnp.exp(jax.random.uniform(key_sequence[4], (BATCH, KV_HEADS, 8), jnp.float32, jnp.log(0.5), jnp.log(2.0)))
    block_multiplier = jnp.repeat(block_multiplier, CACHE_SLOTS // 8, axis=2)
    coarse_multiplier = jax.random.uniform(key_sequence[5], complete_shape, jnp.float32, 0.5, 2.0)
    spike_flag = (jax.random.uniform(key_sequence[6], complete_shape) < 3.0 / CACHE_SLOTS) & sluggish_flag
    spike_penalty = jnp.log(jax.random.uniform(key_sequence[7], complete_shape, jnp.float32, 0.5, 0.8))
    gate_logarithms = -step_frequency * device_multiplier * block_multiplier * coarse_multiplier + jnp.where(spike_flag, spike_penalty, 0.0)
    return jnp.cumsum(gate_logarithms, axis=2)


def block_levels(key, shape, shards, smallest, high):
    loudness, own = 1.0, jax.random.fold_in(key, 6)
    for axis_at, parts in shards:
        heights = jnp.exp(jax.random.uniform(jax.random.fold_in(own, axis_at), (parts,), jnp.float32, smallest / len(shards), high / len(shards)))
        loudness = loudness * jnp.repeat(heights, shape[axis_at] // parts).reshape([-1 if axis == axis_at else 1 for axis in range(len(shape))])
    return loudness


def routed_block(stream_key, own, number, rows, amount, top, reach, slope):
    sequence = jax.random.permutation(stream_key, amount)
    crowded, common = shares(amount, rows * top, reach, slope, True), shares(amount, rows * top, reach, slope, False)
    places = jnp.arange(amount)

    def named(sizes, rotation):
        used = int((sizes > 0).sum())
        fixed = max(1, used // 4)
        shifted = fixed + (places - fixed + rotation * (used - fixed)) % max(1, amount - fixed)
        return jnp.zeros((amount,), jnp.int32).at[sequence[jnp.where(places < fixed, places, shifted)]].set(jnp.asarray(sizes, jnp.int32))

    sizes = jnp.where(number % 4 == 0, named(crowded, number // 4), named(common, number - number // 4 - 1))
    mixed = jax.random.permutation(jax.random.fold_in(own, 3), amount)
    giver, taker = mixed[0:amount // 2 * 2:2], mixed[1:amount // 2 * 2:2]
    slack = jnp.minimum(sizes[giver] - 1, reach - sizes[taker]) // 2
    slack = jnp.where((giver == sequence[0]) | (taker == sequence[0]) | (sizes[taker] == 0), 0, jnp.maximum(slack, 0))
    shifted = jax.random.randint(jax.random.fold_in(own, 4), (amount // 2,), 0, 1 << 20) % (slack + 1)
    sizes = sizes.at[giver].add(-shifted).at[taker].add(shifted)
    members = jnp.searchsorted(jnp.cumsum(sizes), jnp.arange(rows * top), side="right").astype(jnp.int32)
    listing = members.reshape(top, rows).T
    listing = listing[jax.random.permutation(jax.random.fold_in(own, 1), rows)]
    rotation = jax.random.randint(jax.random.fold_in(own, 2), (rows, 1), 0, top)
    return jnp.take_along_axis(listing, (jnp.arange(top)[None, :] + rotation) % top, axis=1)


def shares(number_of, total, reach, lean, full):
    weights = [(1 << 20) // math.isqrt(rank ** lean) + 1 for rank in range(1, number_of + 1)]
    largest = reach if full else min(reach, max(-(-total // number_of), total * weights[0] // sum(weights)))
    least = 1 if total - largest >= number_of - 1 else 0
    given, spare = [largest] + [least] * (number_of - 1), total - largest - least * (number_of - 1)
    while spare > 0:
        candidates = [i for i in range(1, number_of) if given[i] < largest] or [i for i in range(1, number_of) if given[i] < reach]
        whole, budget = sum([weights[i] for i in candidates]), spare
        for i in candidates:
            extra = min(reach - given[i], max(1, budget * weights[i] // whole), spare)
            given[i] = given[i] + extra
            spare = spare - extra
    return np.array(given)


def bell_draw(rng, extent, scale, most, shards=(), held_as=jnp.bfloat16):
    gain = block_levels(rng, extent, shards, -0.22, 0.18) if shards else 1.0
    result = jax.random.normal(rng, extent, jnp.float32) * scale * gain
    return jnp.minimum(jnp.maximum(result, -most), most).astype(held_as)


def setup_inputs(seed: int = 0) -> dict:
    keys = jax.random.split(jax.random.key(seed), 24)
    tokens = bell_draw(keys[0], (BATCH, D), 0.3, 1.796875, ((0, 8),))
    attn_gain = jnp.clip(1.0 + 0.18 * jax.random.normal(keys[1], (D,), jnp.float32), 0.1, 1.9)
    w_query = bell_draw(keys[2], (D, HEADS * HEAD_DIM), D ** -0.5, 0.1875, ((1, 4),))
    w_key = bell_draw(keys[3], (D, KV_HEADS * HEAD_DIM), D ** -0.5, 0.1875, ((1, 4),))
    w_value = bell_draw(keys[4], (D, KV_HEADS * HEAD_DIM), D ** -0.5, 0.1875, ((1, 4),))
    w_forget = bell_draw(keys[5], (D, KV_HEADS), D ** -0.5, 0.1875, ((1, 4),))
    forget_bias = jnp.clip(-1.0 + 3.0 * jax.random.uniform(keys[6], (KV_HEADS,), jnp.float32) ** block_levels(keys[6], (KV_HEADS,), ((0, 4),), -0.2, 0.2), -1.0, 2.0)
    query_gain = jnp.clip(1.0 + 0.18 * jax.random.normal(keys[7], (HEAD_DIM,), jnp.float32), 0.1, 1.9)
    key_gain = jnp.clip(1.0 + 0.18 * jax.random.normal(keys[8], (HEAD_DIM,), jnp.float32), 0.1, 1.9)
    cache_pairs = draw_cache_pairs(jax.random.fold_in(keys[23], 71), 0)
    cache_cum = draw_cache_cum(jax.random.fold_in(keys[23], 71), 0)
    lengths = draw_lengths(jax.random.fold_in(keys[23], 71), 0)
    w_output = bell_draw(keys[12], (HEADS * HEAD_DIM, D), (HEADS * HEAD_DIM) ** -0.5, 0.1875, ((0, 4),))
    ffn_gain = jnp.clip(1.0 + 0.18 * jax.random.normal(keys[13], (D,), jnp.float32), 0.1, 1.9)
    expert_ids_keys = jax.random.split(jax.random.fold_in(keys[14], 1), BATCH // SEQ_GRP)
    expert_ids_turns = jax.random.permutation(jax.random.fold_in(keys[14], 3), BATCH // SEQ_GRP)
    expert_ids = jax.vmap(lambda own, number: routed_block(jax.random.fold_in(keys[14], 2), own, number, SEQ_GRP, EXPERTS, TOP_K, CAP, 2))(expert_ids_keys, expert_ids_turns).reshape((BATCH, TOP_K))
    route_weight = jnp.clip(jax.random.uniform(keys[15], (BATCH, TOP_K), jnp.float32, 0.2, 1.0), 0.2, 1.0)
    w_exp_gate = bell_draw(keys[16], (EXPERTS, D, FF_EXPERT), D ** -0.5, 0.1875, ((0, 8), (2, 4)))
    w_exp_up = bell_draw(keys[17], (EXPERTS, D, FF_EXPERT), D ** -0.5, 0.1875, ((0, 8), (2, 4)))
    w_exp_down = bell_draw(keys[18], (EXPERTS, FF_EXPERT, D), FF_EXPERT ** -0.5, 0.09375, ((0, 8), (1, 4)))
    shared_gate = bell_draw(keys[19], (D,), D ** -0.5, 0.1875)
    w_dense_gate = bell_draw(keys[20], (DENSE_FF, D), D ** -0.5, 0.1875, ((0, 8),))
    w_dense_up = bell_draw(keys[21], (DENSE_FF, D), D ** -0.5, 0.1875, ((0, 8),))
    w_dense_down = bell_draw(keys[22], (DENSE_FF, D), DENSE_FF ** -0.5, 0.09375, ((0, 8), (1, 4)))
    return dict(tokens=tokens, attn_gain=attn_gain, w_query=w_query, w_key=w_key, w_value=w_value, w_forget=w_forget, forget_bias=forget_bias, query_gain=query_gain, key_gain=key_gain, cache_pairs=cache_pairs, cache_cum=cache_cum, lengths=lengths, w_output=w_output, ffn_gain=ffn_gain, expert_ids=expert_ids, route_weight=route_weight, w_exp_gate=w_exp_gate, w_exp_up=w_exp_up, w_exp_down=w_exp_down, shared_gate=shared_gate, w_dense_gate=w_dense_gate, w_dense_up=w_dense_up, w_dense_down=w_dense_down)


EPSILON = 1e-06

def rms_scale(values, gain_row):
    mean_square = lax.optimization_barrier(jnp.mean(values * values, axis=-1, keepdims=True))
    return values * lax.rsqrt(mean_square + EPSILON) * gain_row

def stored(values):
    return lax.optimization_barrier(values.astype(jnp.bfloat16))

def rounded(values):
    return stored(values).astype(jnp.float32)

def attend(per_block):
    query_rows, fresh_key, value_new, now_cum, cache_block, cum_block, length = per_block
    head_size = query_rows.shape[-1]
    position = jnp.arange(cache_block.shape[2], dtype=jnp.int32)
    is_live = position[None, None, :] < length[:, None, None]
    cached_keys = cache_block[..., :head_size].astype(jnp.float32)
    cached_values = cache_block[..., head_size:].astype(jnp.float32)
    score_multiplier = head_size ** (-0.5)
    past_score = jnp.einsum('bkgd,bkld->bkgl', query_rows, cached_keys) * score_multiplier
    past_score = past_score + (now_cum[:, :, None] - cum_block)[:, :, None, :]
    past_score = jnp.where(is_live[:, :, None, :], past_score, -jnp.inf)
    current_score = jnp.einsum('nlte,nle->nlt', query_rows, fresh_key) * score_multiplier
    row_peak = jnp.maximum(lax.optimization_barrier(jnp.max(past_score, axis=3)), current_score)
    past_exp = jnp.exp(past_score - row_peak[..., None])
    own_exp = jnp.exp(current_score - row_peak)
    denom_sum = lax.optimization_barrier(jnp.sum(past_exp, axis=3)) + own_exp
    past_prob = rounded(past_exp / denom_sum[..., None])
    own_prob = rounded(own_exp / denom_sum)
    head_mix = jnp.einsum('bkgl,bkld->bkgd', past_prob, cached_values)
    head_mix = head_mix + own_prob[..., None] * value_new[:, :, None, :]
    return stored(head_mix)

def reference(tokens, attn_gain, w_query, w_key, w_value, w_forget, forget_bias, query_gain, key_gain, cache_pairs, cache_cum, lengths, w_output, ffn_gain, expert_ids, route_weight, w_exp_gate, w_exp_up, w_exp_down, shared_gate, w_dense_gate, w_dense_up, w_dense_down):
    tokens_f = tokens.astype(jnp.float32)
    normed = stored(rms_scale(tokens_f, attn_gain))
    group_size = HEADS // KV_HEADS
    query_raw = jnp.dot(normed, w_query, preferred_element_type=jnp.float32)
    query_rows = rounded(rms_scale(query_raw.reshape(BATCH, KV_HEADS, group_size, HEAD_DIM), query_gain))
    key_raw = jnp.dot(normed, w_key, preferred_element_type=jnp.float32).reshape(BATCH, KV_HEADS, HEAD_DIM)
    fresh_key = rounded(rms_scale(key_raw, key_gain))
    value_new = rounded(jnp.dot(normed, w_value, preferred_element_type=jnp.float32))
    value_new = value_new.reshape(BATCH, KV_HEADS, HEAD_DIM)
    log_gate = jax.nn.log_sigmoid(jnp.dot(normed, w_forget, preferred_element_type=jnp.float32) + forget_bias)
    last_index = jnp.broadcast_to((lengths - 1)[:, None, None], (BATCH, KV_HEADS, 1)).astype(jnp.int32)
    last_cum = jnp.take_along_axis(cache_cum, last_index, axis=2)[:, :, 0]
    now_cum = last_cum + log_gate

    def to_blocks(values):
        return values.reshape((N_EP, SEQ_GRP) + values.shape[1:])
    head_mix = lax.map(attend, tuple((to_blocks(item) for item in (query_rows, fresh_key, value_new, now_cum, cache_pairs, cache_cum, lengths))))
    head_mix = head_mix.reshape(BATCH, HEADS * HEAD_DIM)
    head_span = HEAD_GROUP * HEAD_DIM
    attn_out = jnp.zeros((BATCH, D), jnp.float32)
    for member in range(N_TP):
        partial_value = jnp.dot(head_mix[:, member * head_span:(member + 1) * head_span], w_output[member * head_span:(member + 1) * head_span], preferred_element_type=jnp.float32)
        attn_out = attn_out + rounded(partial_value)
    residual = stored(tokens_f + attn_out)
    residual_f = residual.astype(jnp.float32)
    normed_two = stored(rms_scale(residual_f, ffn_gain))
    grouped_f = normed_two.astype(jnp.float32).reshape(N_EP, SEQ_GRP, D)
    gate_raw = jnp.dot(normed_two, w_dense_gate.T, preferred_element_type=jnp.float32)
    up_raw = jnp.dot(normed_two, w_dense_up.T, preferred_element_type=jnp.float32)
    dense_hidden = stored(jax.nn.silu(gate_raw) * up_raw)
    mix_gate = jax.nn.sigmoid(jnp.dot(normed_two, shared_gate, preferred_element_type=jnp.float32))
    dense_out = mix_gate[:, None] * jnp.dot(dense_hidden, w_dense_down, preferred_element_type=jnp.float32)
    unit_span = FF_EXPERT // N_TP

    def expert_step(running, expert_item):
        member_id, gate_w, up_w, down_w = expert_item
        chosen = expert_ids == member_id
        is_hit = lax.optimization_barrier(jnp.sum(chosen.astype(jnp.int32), axis=1)).reshape(N_EP, SEQ_GRP)
        weight = lax.optimization_barrier(jnp.sum(jnp.where(chosen, route_weight, 0.0), axis=1))
        slot_rank = jnp.cumsum(is_hit, axis=1)
        slot_ids = jnp.arange(1, CAP + 1, dtype=jnp.int32)[None, :, None]
        picker = ((slot_rank[:, None, :] == slot_ids) & (is_hit[:, None, :] == 1)).astype(jnp.float32)
        picked = jnp.einsum('scn,snd->scd', picker, grouped_f).reshape(N_EP * CAP, D).astype(jnp.bfloat16)
        gate_part = jnp.dot(picked, gate_w, preferred_element_type=jnp.float32)
        up_part = jnp.dot(picked, up_w, preferred_element_type=jnp.float32)
        hidden = stored(jax.nn.silu(gate_part) * up_part)
        expert_rows = jnp.zeros((N_EP * CAP, D), jnp.float32)
        for member in range(N_TP):
            partial_value = jnp.dot(hidden[:, member * unit_span:(member + 1) * unit_span], down_w[member * unit_span:(member + 1) * unit_span], preferred_element_type=jnp.float32)
            expert_rows = expert_rows + rounded(partial_value)
        expert_rows = rounded(expert_rows).reshape(N_EP, CAP, D)
        placed = jnp.einsum('scn,scd->snd', picker, expert_rows).reshape(BATCH, D)
        return (running + placed * weight[:, None], None)
    expert_sum = lax.scan(expert_step, jnp.zeros((BATCH, D), jnp.float32), (jnp.arange(EXPERTS, dtype=jnp.int32), w_exp_gate, w_exp_up, w_exp_down))[0]
    return (residual_f + expert_sum + dense_out).astype(jnp.bfloat16)
```

```python
import functools

import jax
import jax.numpy as jnp
from jax import lax
from jax.experimental import pallas as pl
from jax.experimental.pallas import tpu as pltpu
from jax.sharding import PartitionSpec as P

EPSILON = 1e-06
MESH = pl.DeviceIdType.MESH
VMEM_BYTES = 56 * 1024 * 1024


def whole_layer(
    n_ep, n_tp, cap,
    tokens_hbm, attn_gain_hbm, query_gain_hbm, key_gain_hbm, forget_hbm, bias_hbm, length_hbm,
    gain_hbm, ids_hbm, route_hbm, shared_hbm,
    wq_hbm, wk_hbm, wv_hbm, cum_hbm, cache_hbm, wo_hbm,
    wg_hbm, wu_hbm, wd_hbm, dg_hbm, du_hbm, dd_hbm,
    out_ref,
    tokens_ref, attn_gain_ref, query_gain_ref, key_gain_ref, forget_ref, bias_ref, length_ref,
    gain_ref, ids_ref, route_ref, shared_ref,
    wq, wkv, cum, cache, wo_ref, mixed,
    wg, wu, wd, dg, du, dd,
    part_out, part_in, gathered, rows_f, exp_out, exp_in, total, sum_out, sum_in,
    small_sem, attn_sem, load_sem, part_send, part_recv, ring_send, ring_recv, fan_send, fan_recv,
    exp_send, exp_recv, sum_send, sum_recv,
):
    me = lax.axis_index("ep")
    col = lax.axis_index("tp")
    seq_rows, width = tokens_ref.shape
    span = width // n_tp
    slots = n_ep * cap
    batch = n_ep * seq_rows
    f32, bf16 = jnp.float32, jnp.bfloat16
    head = query_gain_ref.shape[1]
    heads = wq.shape[1] // head
    lanes = 2 * head
    eight = 8
    bunch = 4
    small = [
        pltpu.make_async_copy(src, dst, small_sem.at[i])
        for i, (src, dst) in enumerate((
            (tokens_hbm, tokens_ref), (attn_gain_hbm, attn_gain_ref), (wq_hbm, wq),
            (wk_hbm, wkv.at[pl.ds(0, head)]), (wv_hbm, wkv.at[pl.ds(head, head)]),
            (forget_hbm, forget_ref), (bias_hbm, bias_ref), (length_hbm, length_ref),
            (query_gain_hbm, query_gain_ref), (key_gain_hbm, key_gain_ref), (cum_hbm.at[:, 0], cum)))
    ]
    caches = [
        pltpu.make_async_copy(cache_hbm.at[pl.ds(b, bunch), 0], cache.at[pl.ds(b, bunch)], attn_sem.at[b // bunch])
        for b in range(0, seq_rows, bunch)
    ]
    later = [
        pltpu.make_async_copy(src, dst, load_sem.at[i])
        for i, (src, dst) in enumerate((
            (wo_hbm, wo_ref), (gain_hbm, gain_ref), (ids_hbm, ids_ref), (route_hbm, route_ref),
            (shared_hbm, shared_ref), (wg_hbm.at[0], wg), (wu_hbm.at[0], wu), (wd_hbm.at[0], wd),
            (dg_hbm, dg), (du_hbm, du), (dd_hbm, dd)))
    ]
    for load in small + caches + later[:5]:
        load.start()

    barrier = pltpu.get_barrier_semaphore()
    for k in range(1, n_ep):
        pl.semaphore_signal(barrier, inc=1, device_id={"ep": lax.rem(me + k, n_ep)}, device_id_type=MESH)
    for d in range(1, n_tp):
        pl.semaphore_signal(barrier, inc=1, device_id={"tp": lax.rem(col + d, n_tp)}, device_id_type=MESH)

    def columns(d):
        return pl.ds(pl.multiple_of(lax.rem(col + d, n_tp) * span, span), span)

    def to_tp(src, dst, send, recv, d):
        return pltpu.make_async_remote_copy(
            src_ref=src, dst_ref=dst, send_sem=send, recv_sem=recv,
            device_id={"tp": lax.rem(col + d, n_tp)}, device_id_type=MESH)

    def to_ep(src, dst, send, recv, peer):
        return pltpu.make_async_remote_copy(
            src_ref=src, dst_ref=dst, send_sem=send, recv_sem=recv,
            device_id={"ep": peer}, device_id_type=MESH)

    if n_ep == 8:
        deep, side = me // 2, lax.rem(me, 2)
        low = (deep < 2).astype(jnp.int32)
        inner = low * deep + (1 - low) * (3 - deep)
        line = [inner, 1 - inner, 2, 3]
        line = [low * at + (1 - low) * (3 - at) for at in line]
        peers = [line[k // 2] * 2 + (side if k % 2 == 0 else 1 - side) for k in range(n_ep)]
    else:
        peers = [lax.rem(me + k, n_ep) for k in range(n_ep)]
    far_first = list(range(n_ep - 1, 0, -1))

    contract = (((1,), (1,)), ((), ()))

    def iota(shape, axis):
        return lax.broadcasted_iota(jnp.int32, shape, axis).astype(f32)

    def group_of(values, size):
        return jnp.floor((values + 0.5) * (1.0 / size))

    def rms(values, gain):
        return values * lax.rsqrt(jnp.mean(values * values, axis=1, keepdims=True) + EPSILON) * gain

    def rounded(values):
        return values.astype(bf16).astype(f32)

    def half_turn(values):
        return pltpu.roll(values, head, 1)

    left = lax.broadcasted_iota(jnp.int32, (seq_rows, lanes), 1) < head
    small[0].wait()
    small[1].wait()
    token_f = tokens_ref[...].astype(f32)
    normed_one = rms(token_f, attn_gain_ref[...]).astype(bf16)
    small[2].wait()
    query_raw = jnp.dot(normed_one, wq[...], preferred_element_type=f32)
    for load in small[3:10]:
        load.wait()
    pair_raw = lax.dot_general(normed_one, wkv[...], contract, preferred_element_type=f32)
    gate_in = jnp.sum(normed_one.astype(f32) * forget_ref[...].astype(f32), axis=1, keepdims=True) + bias_ref[...]
    log_gate = jnp.minimum(gate_in, 0.0) - jnp.log(1.0 + jnp.exp(-jnp.abs(gate_in)))
    eye = iota((seq_rows, seq_rows), 0) == iota((seq_rows, seq_rows), 1)
    lengths = jnp.sum(jnp.where(eye, jnp.broadcast_to(length_ref[...].astype(f32), (seq_rows, seq_rows)), 0.0), axis=1, keepdims=True)

    def half_scales(values):
        squares = values * values
        first = jnp.sum(jnp.where(left, squares, 0.0), axis=1, keepdims=True)
        second = jnp.sum(jnp.where(left, 0.0, squares), axis=1, keepdims=True)
        return lax.rsqrt(first / head + EPSILON), lax.rsqrt(second / head + EPSILON)

    gain_twice = jnp.concatenate([query_gain_ref[...]] * 2, axis=1)
    queries = []
    for a in range(heads // 2):
        raw = query_raw[:, lanes * a:lanes * (a + 1)]
        first, second = half_scales(raw)
        query = rounded(raw * jnp.where(left, first, second) * gain_twice)
        turned = half_turn(query)
        queries += [jnp.where(left, query, turned), jnp.where(left, turned, query)]
    key_scale, _ = half_scales(pair_raw)
    key_gain = jnp.concatenate([key_gain_ref[...]] * 2, axis=1)
    key = jnp.where(left, rounded(pair_raw * key_scale * key_gain), 0.0)
    value = rounded(pair_raw)
    value = jnp.where(left, half_turn(value), value)
    multiplier = head ** (-0.5)
    own_scores = [jnp.sum(query * key, axis=1, keepdims=True) * multiplier for query in queries]
    scaled = [query * multiplier for query in queries]
    small[10].wait()
    position = iota(cum.shape, 1)
    now = jnp.sum(jnp.where(position == lengths - 1.0, cum[...], 0.0), axis=1, keepdims=True) + log_gate
    cum[...] = jnp.where(position < lengths, now - cum[...], -1e30)

    row = lax.broadcasted_iota(jnp.int32, (eight, lanes), 0)
    left_eight = lax.broadcasted_iota(jnp.int32, (eight, lanes), 1) < head
    key_at = [row == jnp.where(left_eight, 2 * p, 2 * p + 1) for p in range(eight // 2)]
    value_at = [row == jnp.where(left_eight, 2 * p + 1, 2 * p) for p in range(eight // 2)]

    def score_of(i):
        lines = slice(i * eight, (i + 1) * eight)
        lhs = jnp.concatenate([
            jnp.concatenate([jnp.where(key_at[p], query[lines], 0.0) for query in scaled], axis=0)
            for p in range(eight // 2)], axis=1).astype(bf16)
        keys = jnp.concatenate([cache[i * eight + b, :, 0:head] for b in range(eight)], axis=1)
        return lax.dot_general(lhs, keys, contract, preferred_element_type=f32)

    def attend(i, score):
        lines = slice(i * eight, (i + 1) * eight)
        score = score + jnp.concatenate([cum[lines, :]] * heads, axis=0)
        own = jnp.concatenate([values[lines] for values in own_scores], axis=0)
        peak = jnp.maximum(jnp.max(score, axis=1, keepdims=True), own)
        past = jnp.exp(score - peak)
        own = jnp.exp(own - peak)
        inverse = 1.0 / (jnp.sum(past, axis=1, keepdims=True) + own)
        prob = (past * inverse).astype(bf16)
        own = rounded(own * inverse)
        values = jnp.concatenate([cache[i * eight + (b ^ 1), :, head:2 * head] for b in range(eight)], axis=1)
        wide = jnp.dot(prob, values, preferred_element_type=f32)
        mixes = []
        for h in range(heads):
            here = slice(h * eight, (h + 1) * eight)
            mix = sum(jnp.where(value_at[p], wide[here, lanes * p:lanes * (p + 1)], 0.0) for p in range(eight // 2))
            mixes.append(mix + half_turn(mix) + own[here] * value[lines])
        for a in range(heads // 2):
            mixed[lines, lanes * a:lanes * (a + 1)] = jnp.where(left_eight, mixes[2 * a], mixes[2 * a + 1])

    score = None
    for i in range(seq_rows // eight):
        for load in caches[i * eight // bunch:(i + 1) * eight // bunch]:
            load.wait()
        ahead = score_of(i)
        if score is not None:
            attend(i - 1, score)
        score = ahead
    for load in later[5:]:
        load.start()
    attend(seq_rows // eight - 1, score)
    head_mix = mixed[...].astype(bf16)
    later[0].wait()

    for d in range(1, n_tp):
        part_out[d] = jnp.dot(head_mix, wo_ref[:, columns(d)], preferred_element_type=f32).astype(bf16)
    pl.semaphore_wait(barrier, n_ep + n_tp - 2)
    parts = [to_tp(part_out.at[d], part_in.at[d], part_send.at[d], part_recv.at[d], d) for d in range(1, n_tp)]
    for copy in parts:
        copy.start()
    own = jnp.dot(head_mix, wo_ref[:, columns(0)], preferred_element_type=f32)
    attn = rounded(own)
    token_block = tokens_ref[:, columns(0)].astype(f32)
    for copy in parts:
        copy.wait_recv()
    for d in range(1, n_tp):
        attn = attn + part_in[d].astype(f32)
    residual = (token_block + attn).astype(bf16)
    gathered[col, me] = residual

    rings = [to_ep(gathered.at[col, me], gathered.at[col, me], ring_send.at[k], ring_recv.at[me], peers[k]) for k in far_first]
    for copy in rings:
        copy.start()
    fans = []
    if n_tp == 4:
        beside = col + 1 - 2 * lax.rem(col, 2)
        across = lax.rem(col + 2, 4)
        routes, first = ((col, across), (col, beside), (across, beside)), 2
    else:
        routes, first = tuple((col, lax.rem(col + d, n_tp)) for d in range(1, n_tp)), n_tp - 1

    def fan_copies(k, slot):
        return [
            pltpu.make_async_remote_copy(
                src_ref=gathered.at[block, slot], dst_ref=gathered.at[block, slot],
                send_sem=fan_send.at[k, d], recv_sem=fan_recv.at[k, d],
                device_id={"tp": target}, device_id_type=MESH)
            for d, (block, target) in enumerate(routes)
        ]

    def arrive(k):
        slot = peers[k]
        if k > 0:
            to_ep(gathered.at[col, slot], gathered.at[col, slot], ring_send.at[k], ring_recv.at[slot], slot).wait_recv()
        fan = fan_copies(k, slot)
        for copy in fan[:first]:
            copy.start()
        fans.append(fan)

    arrive(0)
    for load in later[1:5]:
        load.wait()
    expert = me
    hit = jnp.zeros((1, batch), f32)
    weight_row = jnp.zeros((1, batch), f32)
    for k in range(ids_ref.shape[0]):
        same = ids_ref[k:k + 1, :] == expert
        hit = hit + jnp.where(same, 1.0, 0.0)
        weight_row = weight_row + jnp.where(same, route_ref[k:k + 1, :], 0.0)
    row_at = iota((batch, batch), 0)
    col_at = iota((batch, batch), 1)
    before = (row_at <= col_at) & (row_at >= group_of(col_at, seq_rows) * seq_rows)
    hits = jnp.broadcast_to(hit, (8, batch))
    rank = jnp.dot(hits.astype(bf16), before.astype(f32).astype(bf16), preferred_element_type=f32)[0:1]
    slot_of = jnp.where((hit > 0.5) & (rank < cap + 0.5), group_of(iota((1, batch), 1), seq_rows) * cap + rank - 1.0, -1.0)
    pick_f = jnp.where(iota((slots, batch), 0) == slot_of, 1.0, 0.0)
    pick = pick_f.astype(bf16)
    place = pick_f.T.astype(bf16)
    weight = jnp.sum((pick_f * weight_row).T, axis=1, keepdims=True)
    for k in range(1, n_ep):
        arrive(k)

    for k in range(n_ep + 1):
        if k < n_ep and first < len(routes):
            fans[k][0].wait_recv()
            fans[k][2].start()
        k = k - 1
        if k < 0:
            continue
        for copy in (fans[k][1:] if first < len(routes) else fans[k]):
            copy.wait_recv()
        slot = peers[k]
        blocks = [gathered[t, slot].astype(f32) for t in range(n_tp)]
        squares = sum(jnp.sum(b * b, axis=1, keepdims=True) for b in blocks)
        scale = lax.rsqrt(squares / width + EPSILON)
        for t in range(n_tp):
            rows_f[pl.ds(pl.multiple_of(slot * seq_rows, 8), seq_rows), t * span:(t + 1) * span] = (
                blocks[t] * scale * gain_ref[:, t * span:(t + 1) * span])
    normed = rows_f[...].astype(bf16)

    picked = jnp.dot(pick, normed, preferred_element_type=f32).astype(bf16)
    for load in later[5:8]:
        load.wait()
    gate = jnp.dot(picked, wg[...], preferred_element_type=f32)
    up = jnp.dot(picked, wu[...], preferred_element_type=f32)
    hidden = (gate / (1.0 + jnp.exp(-gate)) * up).astype(bf16)
    moves = []
    for d in sorted(range(1, n_tp), key=lambda d: d != 2):
        exp_out[d] = jnp.dot(hidden, wd[:, columns(d)], preferred_element_type=f32).astype(bf16)
        copy = to_tp(exp_out.at[d], exp_in.at[d], exp_send.at[d], exp_recv.at[d], d)
        copy.start()
        moves.append(copy)
    expert_rows = rounded(jnp.dot(hidden, wd[:, columns(0)], preferred_element_type=f32))

    shared_tiles = shared_ref[...].astype(f32)
    shared = jnp.concatenate([shared_tiles[i:i + 1] for i in range(width // 128)], axis=1)
    for load in later[8:]:
        load.wait()
    step = seq_rows * 8 if n_ep % 8 == 0 else batch

    def dense(at):
        rows = rows_f[pl.ds(at, step), :].astype(bf16)
        gate = lax.dot_general(rows, dg[...], contract, preferred_element_type=f32)
        up = lax.dot_general(rows, du[...], contract, preferred_element_type=f32)
        hidden = (gate / (1.0 + jnp.exp(-gate)) * up).astype(bf16)
        mix = jnp.sum(rows.astype(f32) * shared, axis=1, keepdims=True)
        mix = 1.0 / (1.0 + jnp.exp(-mix))
        total[pl.ds(at, step), :] = mix * jnp.dot(hidden, dd[...], preferred_element_type=f32)

    if step == batch:
        dense(0)
    else:
        @pl.loop(0, batch // step)
        def _(i):
            dense(pl.multiple_of(i * step, step))

    for copy in moves:
        copy.wait_recv()
    for d in range(1, n_tp):
        expert_rows = expert_rows + exp_in[d].astype(f32)
    placed = jnp.dot(place, expert_rows.astype(bf16), preferred_element_type=f32)
    total[...] = total[...] + placed * weight

    sums = []
    for k in far_first:
        slot = peers[k]
        sum_out[k] = total[pl.ds(pl.multiple_of(slot * seq_rows, 8), seq_rows), :].astype(bf16)
        copy = to_ep(sum_out.at[k], sum_in.at[me], sum_send.at[k], sum_recv.at[me], slot)
        copy.start()
        sums.append(copy)
    result = residual.astype(f32) + total[pl.ds(pl.multiple_of(me * seq_rows, 8), seq_rows), :]
    for k in range(1, n_ep):
        slot = peers[k]
        to_ep(sum_out.at[k], sum_in.at[slot], sum_send.at[k], sum_recv.at[slot], slot).wait_recv()
        result = result + sum_in[slot].astype(f32)
    out_ref[...] = result.astype(bf16)
    for copy in parts + rings + [c for fan in fans for c in fan] + moves + sums:
        copy.wait_send()


def layer_call(tokens, attn_gain, w_query, w_key, w_value, w_forget, forget_bias, query_gain, key_gain,
              cache_pairs, cache_cum, lengths, w_output, ffn_gain, expert_ids, route_weight, shared_gate,
              w_exp_gate, w_exp_up, w_exp_down, w_dense_gate, w_dense_up, w_dense_down):
    n_ep, n_tp = lax.axis_size("ep"), lax.axis_size("tp")
    seq_rows, width = tokens.shape
    cap = max(2, min(seq_rows, 128 // n_ep))
    span = width // n_tp
    slots, batch = n_ep * cap, n_ep * seq_rows
    bf16, f32 = jnp.bfloat16, jnp.float32
    vmem = pl.BlockSpec(memory_space=pltpu.VMEM)
    hbm = pl.BlockSpec(memory_space=pltpu.HBM)
    dma = pltpu.SemaphoreType.DMA
    return pl.pallas_call(
        functools.partial(whole_layer, n_ep, n_tp, cap),
        out_shape=pltpu.VMEM((seq_rows, span), bf16),
        in_specs=[hbm] * 23,
        out_specs=vmem,
        scratch_shapes=[
            pltpu.VMEM(tokens.shape, bf16),
            pltpu.VMEM((1, width), f32),
            pltpu.VMEM((1, query_gain.shape[0]), f32),
            pltpu.VMEM((1, key_gain.shape[0]), f32),
            pltpu.VMEM((1, width), bf16),
            pltpu.VMEM((1, 1), f32),
            pltpu.VMEM((1, seq_rows), jnp.int32),
            pltpu.VMEM((1, width), f32),
            pltpu.VMEM(expert_ids.shape[::-1], jnp.int32),
            pltpu.VMEM(route_weight.shape[::-1], f32),
            pltpu.VMEM((width // 128, 128), bf16),
            pltpu.VMEM(w_query.shape, bf16),
            pltpu.VMEM((2 * w_key.shape[1], width), bf16),
            pltpu.VMEM((seq_rows, cache_cum.shape[2]), f32),
            pltpu.VMEM((seq_rows,) + cache_pairs.shape[2:], bf16),
            pltpu.VMEM(w_output.shape, bf16),
            pltpu.VMEM((seq_rows, w_query.shape[1]), f32),
            pltpu.VMEM(w_exp_gate.shape[1:], bf16),
            pltpu.VMEM(w_exp_up.shape[1:], bf16),
            pltpu.VMEM(w_exp_down.shape[1:], bf16),
            pltpu.VMEM(w_dense_gate.shape, bf16),
            pltpu.VMEM(w_dense_up.shape, bf16),
            pltpu.VMEM(w_dense_down.shape, bf16),
            pltpu.VMEM((n_tp, seq_rows, span), bf16),
            pltpu.VMEM((n_tp, seq_rows, span), bf16),
            pltpu.VMEM((n_tp, n_ep, seq_rows, span), bf16),
            pltpu.VMEM((batch, width), f32),
            pltpu.VMEM((n_tp, slots, span), bf16),
            pltpu.VMEM((n_tp, slots, span), bf16),
            pltpu.VMEM((batch, span), f32),
            pltpu.VMEM((n_ep, seq_rows, span), bf16),
            pltpu.VMEM((n_ep, seq_rows, span), bf16),
            dma((11,)),
            dma((seq_rows // 4,)),
            dma((11,)),
            dma((n_tp,)), dma((n_tp,)),
            dma((n_ep,)), dma((n_ep,)),
            dma((n_ep, n_tp)), dma((n_ep, n_tp)),
            dma((n_tp,)), dma((n_tp,)),
            dma((n_ep,)), dma((n_ep,)),
        ],
        compiler_params=pltpu.CompilerParams(
            collective_id=0, has_side_effects=True, vmem_limit_bytes=VMEM_BYTES),
        name="whole_layer",
    )(tokens, attn_gain.reshape(1, width), query_gain.reshape(1, -1), key_gain.reshape(1, -1),
      w_forget.reshape(1, width), forget_bias.reshape(1, 1), lengths.reshape(1, seq_rows),
      ffn_gain.reshape(1, width), expert_ids.T, route_weight.T, shared_gate.reshape(width // 128, 128),
      w_query, w_key.T, w_value.T, cache_cum, cache_pairs, w_output,
      w_exp_gate, w_exp_up, w_exp_down,
      w_dense_gate, w_dense_up, w_dense_down)


def shards(
    tokens,
    attn_gain,
    w_query,
    w_key,
    w_value,
    w_forget,
    forget_bias,
    query_gain,
    key_gain,
    cache_pairs,
    cache_cum,
    lengths,
    w_output,
    ffn_gain,
    expert_ids,
    route_weight,
    w_exp_gate,
    w_exp_up,
    w_exp_down,
    shared_gate,
    w_dense_gate,
    w_dense_up,
    w_dense_down,
):
    return layer_call(
        tokens, attn_gain, w_query, w_key, w_value, w_forget, forget_bias, query_gain, key_gain,
        cache_pairs, cache_cum, lengths, w_output, ffn_gain, expert_ids, route_weight, shared_gate,
        w_exp_gate, w_exp_up, w_exp_down, w_dense_gate, w_dense_up, w_dense_down,
    )


def solution(mesh):
    in_specs = (
        P("ep", None),
        P(),
        P(None, "tp"),
        P(None, "tp"),
        P(None, "tp"),
        P(None, "tp"),
        P("tp"),
        P(),
        P(),
        P("ep", "tp", None, None),
        P("ep", "tp", None),
        P("ep"),
        P("tp", None),
        P(),
        P(),
        P(),
        P("ep", None, "tp"),
        P("ep", None, "tp"),
        P("ep", "tp", None),
        P(),
        P("ep", None),
        P("ep", None),
        P("ep", "tp"),
    )
    out_specs = P("ep", "tp")
    return jax.shard_map(shards, mesh=mesh, in_specs=in_specs, out_specs=out_specs, check_vma=False)
```

```python
import functools

import jax
import jax.numpy as jnp
from jax import lax
from jax.experimental import pallas as pl
from jax.experimental.pallas import tpu as pltpu
from jax.sharding import PartitionSpec as P

EPSILON = 1e-06
MESH = pl.DeviceIdType.MESH
VMEM_BYTES = 56 * 1024 * 1024


def whole_layer(
    n_ep, n_tp, cap,
    tokens_hbm, attn_gain_hbm, query_gain_hbm, key_gain_hbm, forget_hbm, bias_hbm, length_hbm,
    gain_hbm, ids_hbm, route_hbm, shared_hbm,
    wq_hbm, wk_hbm, wv_hbm, cum_hbm, cache_hbm, wo_hbm,
    wg_hbm, wu_hbm, wd_hbm, dg_hbm, du_hbm, dd_hbm,
    out_ref,
    tokens_ref, attn_gain_ref, query_gain_ref, key_gain_ref, forget_ref, bias_ref, length_ref,
    gain_ref, ids_ref, route_ref, shared_ref,
    wq, wkv, cum, cache, wo_ref, mixed,
    wg, wu, wd, dg, du, dd,
    part_out, part_in, gathered, rows_f, pick_ref, place_ref, weight_ref, exp_out, exp_in, total, sum_out, sum_in,
    small_sem, attn_sem, load_sem, part_send, part_recv, ring_send, ring_recv, fan_send, fan_recv, cross_recv,
    exp_send, exp_recv, sum_send, sum_recv,
):
    me = lax.axis_index("ep")
    col = lax.axis_index("tp")
    seq_rows, width = tokens_ref.shape
    span = width // n_tp
    slots = n_ep * cap
    batch = n_ep * seq_rows
    f32, bf16 = jnp.float32, jnp.bfloat16
    head = query_gain_ref.shape[1]
    heads = wq.shape[1] // head
    lanes = 2 * head
    eight = 8
    bunch = eight
    small = [
        pltpu.make_async_copy(src, dst, small_sem.at[i])
        for i, (src, dst) in enumerate((
            (tokens_hbm, tokens_ref), (attn_gain_hbm, attn_gain_ref), (wq_hbm, wq),
            (wk_hbm, wkv.at[pl.ds(0, head)]), (wv_hbm, wkv.at[pl.ds(head, head)]),
            (forget_hbm, forget_ref), (bias_hbm, bias_ref), (length_hbm, length_ref),
            (query_gain_hbm, query_gain_ref), (key_gain_hbm, key_gain_ref), (cum_hbm.at[:, 0], cum)))
    ]
    caches = [
        pltpu.make_async_copy(cache_hbm.at[pl.ds(b, bunch), 0], cache.at[pl.ds(b, bunch)], attn_sem.at[b // bunch])
        for b in range(0, seq_rows, bunch)
    ]
    later = [
        pltpu.make_async_copy(src, dst, load_sem.at[i])
        for i, (src, dst) in enumerate((
            (wo_hbm, wo_ref), (gain_hbm, gain_ref), (ids_hbm, ids_ref), (route_hbm, route_ref),
            (shared_hbm, shared_ref), (wg_hbm.at[0], wg), (wu_hbm.at[0], wu), (wd_hbm.at[0], wd),
            (dg_hbm, dg), (du_hbm, du), (dd_hbm, dd)))
    ]
    for load in small + caches + later[:5]:
        load.start()

    barrier = pltpu.get_barrier_semaphore()
    for k in range(1, n_ep):
        pl.semaphore_signal(barrier, inc=1, device_id={"ep": lax.rem(me + k, n_ep)}, device_id_type=MESH)
    for d in range(1, n_tp):
        pl.semaphore_signal(barrier, inc=1, device_id={"tp": lax.rem(col + d, n_tp)}, device_id_type=MESH)

    def columns(d):
        return pl.ds(pl.multiple_of(lax.rem(col + d, n_tp) * span, span), span)

    def to_tp(src, dst, send, recv, d):
        return pltpu.make_async_remote_copy(
            src_ref=src, dst_ref=dst, send_sem=send, recv_sem=recv,
            device_id={"tp": lax.rem(col + d, n_tp)}, device_id_type=MESH)

    def to_ep(src, dst, send, recv, peer):
        return pltpu.make_async_remote_copy(
            src_ref=src, dst_ref=dst, send_sem=send, recv_sem=recv,
            device_id={"ep": peer}, device_id_type=MESH)

    if n_ep == 8:
        deep, side = me // 2, lax.rem(me, 2)
        low = (deep < 2).astype(jnp.int32)
        inner = low * deep + (1 - low) * (3 - deep)
        line = [inner, 1 - inner, 2, 3]
        line = [low * at + (1 - low) * (3 - at) for at in line]
        peers = [line[k // 2] * 2 + (side if k % 2 == 0 else 1 - side) for k in range(n_ep)]
    else:
        peers = [lax.rem(me + k, n_ep) for k in range(n_ep)]
    sets = [list(range(4)), list(range(4, 8))] if n_ep == 8 else [list(range(n_ep))]
    far_first = list(range(n_ep - 1, 0, -1))

    contract = (((1,), (1,)), ((), ()))

    def iota(shape, axis):
        return lax.broadcasted_iota(jnp.int32, shape, axis).astype(f32)

    def group_of(values, size):
        return jnp.floor((values + 0.5) * (1.0 / size))

    def rms(values, gain):
        return values * lax.rsqrt(jnp.mean(values * values, axis=1, keepdims=True) + EPSILON) * gain

    def rounded(values):
        return values.astype(bf16).astype(f32)

    def half_turn(values):
        return pltpu.roll(values, head, 1)

    left = lax.broadcasted_iota(jnp.int32, (seq_rows, lanes), 1) < head
    small[0].wait()
    small[1].wait()
    token_f = tokens_ref[...].astype(f32)
    normed_one = rms(token_f, attn_gain_ref[...]).astype(bf16)
    small[2].wait()
    query_raw = jnp.dot(normed_one, wq[...], preferred_element_type=f32)
    for load in small[3:10]:
        load.wait()
    pair_raw = lax.dot_general(normed_one, wkv[...], contract, preferred_element_type=f32)
    gate_in = jnp.sum(normed_one.astype(f32) * forget_ref[...].astype(f32), axis=1, keepdims=True) + bias_ref[...]
    log_gate = jnp.minimum(gate_in, 0.0) - jnp.log(1.0 + jnp.exp(-jnp.abs(gate_in)))
    eye = iota((seq_rows, seq_rows), 0) == iota((seq_rows, seq_rows), 1)
    lengths = jnp.sum(jnp.where(eye, jnp.broadcast_to(length_ref[...].astype(f32), (seq_rows, seq_rows)), 0.0), axis=1, keepdims=True)

    def half_scales(values):
        squares = values * values
        first = jnp.sum(jnp.where(left, squares, 0.0), axis=1, keepdims=True)
        second = jnp.sum(jnp.where(left, 0.0, squares), axis=1, keepdims=True)
        return lax.rsqrt(first / head + EPSILON), lax.rsqrt(second / head + EPSILON)

    gain_twice = jnp.concatenate([query_gain_ref[...]] * 2, axis=1)
    queries = []
    for a in range(heads // 2):
        raw = query_raw[:, lanes * a:lanes * (a + 1)]
        first, second = half_scales(raw)
        query = rounded(raw * jnp.where(left, first, second) * gain_twice)
        turned = half_turn(query)
        queries += [jnp.where(left, query, turned), jnp.where(left, turned, query)]
    key_scale, _ = half_scales(pair_raw)
    key_gain = jnp.concatenate([key_gain_ref[...]] * 2, axis=1)
    key = jnp.where(left, rounded(pair_raw * key_scale * key_gain), 0.0)
    value = rounded(pair_raw)
    value = jnp.where(left, half_turn(value), value)
    multiplier = head ** (-0.5)
    own_scores = [jnp.sum(query * key, axis=1, keepdims=True) * multiplier for query in queries]
    scaled = [query * multiplier for query in queries]
    small[10].wait()
    position = iota(cum.shape, 1)
    now = jnp.sum(jnp.where(position == lengths - 1.0, cum[...], 0.0), axis=1, keepdims=True) + log_gate
    cum[...] = jnp.where(position < lengths, now - cum[...], -1e30)

    row = lax.broadcasted_iota(jnp.int32, (eight, lanes), 0)
    left_eight = lax.broadcasted_iota(jnp.int32, (eight, lanes), 1) < head
    key_at = [row == jnp.where(left_eight, 2 * p, 2 * p + 1) for p in range(eight // 2)]
    value_at = [row == jnp.where(left_eight, 2 * p + 1, 2 * p) for p in range(eight // 2)]

    def score_of(i):
        lines = slice(i * eight, (i + 1) * eight)
        lhs = jnp.concatenate([
            jnp.concatenate([jnp.where(key_at[p], query[lines], 0.0) for query in scaled], axis=0)
            for p in range(eight // 2)], axis=1).astype(bf16)
        keys = jnp.concatenate([cache[i * eight + b, :, 0:head] for b in range(eight)], axis=1)
        return lax.dot_general(lhs, keys, contract, preferred_element_type=f32)

    def attend(i, score):
        lines = slice(i * eight, (i + 1) * eight)
        score = score + jnp.concatenate([cum[lines, :]] * heads, axis=0)
        own = jnp.concatenate([values[lines] for values in own_scores], axis=0)
        peak = jnp.maximum(jnp.max(score, axis=1, keepdims=True), own)
        past = jnp.exp(score - peak)
        own = jnp.exp(own - peak)
        inverse = 1.0 / (jnp.sum(past, axis=1, keepdims=True) + own)
        prob = (past * inverse).astype(bf16)
        own = rounded(own * inverse)
        values = jnp.concatenate([cache[i * eight + (b ^ 1), :, head:2 * head] for b in range(eight)], axis=1)
        wide = jnp.dot(prob, values, preferred_element_type=f32)
        mixes = []
        for h in range(heads):
            here = slice(h * eight, (h + 1) * eight)
            mix = sum(jnp.where(value_at[p], wide[here, lanes * p:lanes * (p + 1)], 0.0) for p in range(eight // 2))
            mixes.append(mix + half_turn(mix) + own[here] * value[lines])
        for a in range(heads // 2):
            mixed[lines, lanes * a:lanes * (a + 1)] = jnp.where(left_eight, mixes[2 * a], mixes[2 * a + 1])

    score = None
    for i in range(seq_rows // eight):
        for load in caches[i * eight // bunch:(i + 1) * eight // bunch]:
            load.wait()
        ahead = score_of(i)
        if score is not None:
            attend(i - 1, score)
        score = ahead
    for load in later[5:]:
        load.start()
    attend(seq_rows // eight - 1, score)
    head_mix = mixed[...].astype(bf16)
    later[0].wait()

    partial = jnp.dot(head_mix, wo_ref[...], preferred_element_type=f32).astype(bf16)
    for j in range(n_tp):
        part_out[j] = partial[:, j * span:(j + 1) * span]
    pl.semaphore_wait(barrier, n_ep + n_tp - 2)
    for d in range(1, n_tp):
        there = lax.rem(col + d, n_tp)
        to_tp(part_out.at[there], part_in.at[col], part_send, part_recv, d).start()
    some = pl.ds(0, n_tp - 1)
    parts = to_tp(part_out.at[some], part_in.at[some], part_send, part_recv, 1)
    token_block = tokens_ref[:, columns(0)].astype(f32)
    part_in[col] = part_out[col]
    parts.wait_recv()
    attn = part_in[0].astype(f32)
    for j in range(1, n_tp):
        attn = attn + part_in[j].astype(f32)
    residual = (token_block + attn).astype(bf16)
    gathered[col, me] = residual

    for k in far_first:
        to_ep(gathered.at[col, me], gathered.at[col, me], ring_send, ring_recv.at[me], peers[k]).start()
    if n_tp == 4:
        across, beside = lax.rem(col + 2, 4), col + 1 - 2 * lax.rem(col, 2)
        others = [across, lax.rem(col + 2, 4) + 1 - 2 * lax.rem(col, 2), beside]
        relayed = [k for k in range(n_ep) if k < 0]
    else:
        across, beside = col, col
        others = [lax.rem(col + d, n_tp) for d in range(1, n_tp)]
        relayed = []

    def to_other(block, slot, recv, other):
        return pltpu.make_async_remote_copy(
            src_ref=gathered.at[block, slot], dst_ref=gathered.at[block, slot],
            send_sem=fan_send, recv_sem=recv, device_id={"tp": other}, device_id_type=MESH)

    def arrive(k):
        slot = peers[k]
        if k > 0:
            to_ep(gathered.at[col, slot], gathered.at[col, slot], ring_send, ring_recv.at[slot], slot).wait_recv()
        if k in relayed:
            to_other(col, slot, cross_recv.at[k], across).start()
            to_other(col, slot, fan_recv.at[k], beside).start()
        else:
            for other in others:
                to_other(col, slot, fan_recv.at[k], other).start()

    def relay(k):
        to_other(col, peers[k], cross_recv.at[k], across).wait_recv()
        to_other(across, peers[k], fan_recv.at[k], beside).start()

    def spread(k, blocks):
        group = gathered.at[pl.ds(0, blocks), peers[k]]
        return pltpu.make_async_remote_copy(
            src_ref=group, dst_ref=group, send_sem=fan_send, recv_sem=fan_recv.at[k],
            device_id={"tp": others[0]}, device_id_type=MESH)

    arrive(0)
    for load in later[1:5]:
        load.wait()
    expert = me
    hit = jnp.zeros((1, batch), f32)
    weight_row = jnp.zeros((1, batch), f32)
    for k in range(ids_ref.shape[0]):
        same = ids_ref[k:k + 1, :] == expert
        hit = hit + jnp.where(same, 1.0, 0.0)
        weight_row = weight_row + jnp.where(same, route_ref[k:k + 1, :], 0.0)
    row_at = iota((batch, batch), 0)
    col_at = iota((batch, batch), 1)
    hits = jnp.broadcast_to(hit, (8, batch)).astype(bf16)
    if len(sets) > 1:
        lane = iota((1, batch), 1)
        block = group_of(lane, seq_rows)
        source = lane - block * seq_rows
        for k in range(n_ep):
            source = source + jnp.where(block == k, (peers[k] * seq_rows).astype(f32), 0.0)
        turn = jnp.where(row_at == source, 1.0, 0.0)
        hits = jnp.dot(hits, turn.astype(bf16), preferred_element_type=f32).astype(bf16)
        weight_row = jnp.dot(
            jnp.broadcast_to(weight_row, (8, batch)), turn,
            precision=lax.Precision.HIGHEST, preferred_element_type=f32)[0:1]
    hit = hits[0:1].astype(f32)
    before = (row_at <= col_at) & (row_at >= group_of(col_at, seq_rows) * seq_rows)
    rank = jnp.dot(hits, before.astype(f32).astype(bf16), preferred_element_type=f32)[0:1]
    slot_of = jnp.where((hit > 0.5) & (rank < cap + 0.5), group_of(iota((1, batch), 1), seq_rows) * cap + rank - 1.0, -1.0)
    for n, chosen in enumerate(sets):
        lines = len(chosen) * seq_rows
        places = len(chosen) * cap
        here = slot_of[:, n * lines:(n + 1) * lines]
        pick = jnp.where(iota((places, lines), 0) + n * places == here, 1.0, 0.0)
        pick_ref[n] = pick.astype(bf16)
        place_ref[n] = pick.T.astype(bf16)
        weight_ref[n] = jnp.sum((pick * weight_row[:, n * lines:(n + 1) * lines]).T, axis=1, keepdims=True)
    shared_tiles = shared_ref[...].astype(f32)
    shared = jnp.concatenate([shared_tiles[i:i + 1] for i in range(width // 128)], axis=1)

    def lines_of(k):
        at = k * seq_rows if len(sets) > 1 else pl.multiple_of(peers[k] * seq_rows, 8)
        return pl.ds(at, seq_rows)

    def normalize(k):
        blocks = [gathered[t, peers[k]].astype(f32) for t in range(n_tp)]
        squares = sum(jnp.sum(b * b, axis=1, keepdims=True) for b in blocks)
        scale = lax.rsqrt(squares / width + EPSILON)
        for t in range(n_tp):
            rows_f[lines_of(k), t * span:(t + 1) * span] = (
                blocks[t] * scale * gain_ref[:, t * span:(t + 1) * span])

    def expert_part(n, chosen):
        lines = len(chosen) * seq_rows
        rows = rows_f[n * lines:(n + 1) * lines, :].astype(bf16)
        picked = jnp.dot(pick_ref[n], rows, preferred_element_type=f32).astype(bf16)
        gate = jnp.dot(picked, wg[...], preferred_element_type=f32)
        up = jnp.dot(picked, wu[...], preferred_element_type=f32)
        hidden = (gate / (1.0 + jnp.exp(-gate)) * up).astype(bf16)
        down = jnp.dot(hidden, wd[...], preferred_element_type=f32).astype(bf16)
        for j in range(n_tp):
            exp_out[n, j] = down[:, j * span:(j + 1) * span]
        for d in sorted(range(1, n_tp), key=lambda d: d != 2):
            there = lax.rem(col + d, n_tp)
            to_tp(exp_out.at[n, there], exp_in.at[n, col], exp_send.at[n], exp_recv.at[n], d).start()
        exp_in[n, col] = exp_out[n, col]

    def moves(n):
        there = pl.ds(0, n_tp - 1)
        return to_tp(exp_out.at[n, there], exp_in.at[n, there], exp_send.at[n], exp_recv.at[n], 1)

    def dense(rows):
        rows = rows.astype(bf16)
        gate = lax.dot_general(rows, dg[...], contract, preferred_element_type=f32)
        up = lax.dot_general(rows, du[...], contract, preferred_element_type=f32)
        hidden = (gate / (1.0 + jnp.exp(-gate)) * up).astype(bf16)
        mix = jnp.sum(rows.astype(f32) * shared, axis=1, keepdims=True)
        mix = 1.0 / (1.0 + jnp.exp(-mix))
        return mix * jnp.dot(hidden, dd[...], preferred_element_type=f32)

    def finish(n, chosen):
        moves(n).wait_recv()
        rows = exp_in[n, 0].astype(f32)
        for j in range(1, n_tp):
            rows = rows + exp_in[n, j].astype(f32)
        placed = jnp.dot(place_ref[n], rows.astype(bf16), preferred_element_type=f32) * weight_ref[n]
        lines = len(chosen) * seq_rows
        total[n * lines:(n + 1) * lines, :] = total[n * lines:(n + 1) * lines, :] + placed
        for k in reversed(chosen):
            if k > 0:
                sum_out[k] = total[lines_of(k), :].astype(bf16)
        for k in reversed(chosen):
            if k > 0:
                to_ep(sum_out.at[k], sum_in.at[me], sum_send, sum_recv.at[me], peers[k]).start()

    for k in range(1, n_ep):
        arrive(k)
        if k - 4 in relayed:
            relay(k - 4)
    for load in later[5:]:
        load.wait()
    for n, chosen in enumerate(sets):
        for k in chosen:
            if k > n_ep - 1 - 4 and k in relayed:
                relay(k)
            spread(k, 2 if k in relayed else n_tp - 1).wait_recv()
        for k in chosen:
            normalize(k)
        expert_part(n, chosen)
    step = seq_rows * 8 if n_ep % 8 == 0 else batch
    if step == batch:
        total[...] = dense(rows_f[...])
    else:
        @pl.loop(0, batch // step)
        def _(i):
            at = pl.multiple_of(i * step, step)
            total[pl.ds(at, step), :] = dense(rows_f[pl.ds(at, step), :])
    for n, chosen in enumerate(sets):
        finish(n, chosen)
    result = residual.astype(f32) + total[lines_of(0), :]
    for k in range(1, n_ep):
        slot = peers[k]
        to_ep(sum_out.at[k], sum_in.at[slot], sum_send, sum_recv.at[slot], slot).wait_recv()
        result = result + sum_in[slot].astype(f32)
    out_ref[...] = result.astype(bf16)
    parts.wait_send()
    others_of = gathered.at[0, pl.ds(0, n_ep - 1)]
    to_ep(others_of, others_of, ring_send, ring_recv.at[0], peers[1]).wait_send()
    for k in range(n_ep):
        spread(k, n_tp - 1).wait_send()
    for n in range(len(sets)):
        moves(n).wait_send()
    to_ep(sum_out.at[pl.ds(1, n_ep - 1)], sum_in.at[pl.ds(1, n_ep - 1)], sum_send, sum_recv.at[1], peers[1]).wait_send()


def layer_call(tokens, attn_gain, w_query, w_key, w_value, w_forget, forget_bias, query_gain, key_gain,
              cache_pairs, cache_cum, lengths, w_output, ffn_gain, expert_ids, route_weight, shared_gate,
              w_exp_gate, w_exp_up, w_exp_down, w_dense_gate, w_dense_up, w_dense_down):
    n_ep, n_tp = lax.axis_size("ep"), lax.axis_size("tp")
    seq_rows, width = tokens.shape
    cap = max(2, min(seq_rows, 128 // n_ep))
    n_sets = 2 if n_ep == 8 else 1
    span = width // n_tp
    slots, batch = n_ep * cap, n_ep * seq_rows
    bf16, f32 = jnp.bfloat16, jnp.float32
    vmem = pl.BlockSpec(memory_space=pltpu.VMEM)
    hbm = pl.BlockSpec(memory_space=pltpu.HBM)
    dma = pltpu.SemaphoreType.DMA
    return pl.pallas_call(
        functools.partial(whole_layer, n_ep, n_tp, cap),
        out_shape=pltpu.VMEM((seq_rows, span), bf16),
        in_specs=[hbm] * 23,
        out_specs=vmem,
        scratch_shapes=[
            pltpu.VMEM(tokens.shape, bf16),
            pltpu.VMEM((1, width), f32),
            pltpu.VMEM((1, query_gain.shape[0]), f32),
            pltpu.VMEM((1, key_gain.shape[0]), f32),
            pltpu.VMEM((1, width), bf16),
            pltpu.VMEM((1, 1), f32),
            pltpu.VMEM((1, seq_rows), jnp.int32),
            pltpu.VMEM((1, width), f32),
            pltpu.VMEM(expert_ids.shape[::-1], jnp.int32),
            pltpu.VMEM(route_weight.shape[::-1], f32),
            pltpu.VMEM((width // 128, 128), bf16),
            pltpu.VMEM(w_query.shape, bf16),
            pltpu.VMEM((2 * w_key.shape[1], width), bf16),
            pltpu.VMEM((seq_rows, cache_cum.shape[2]), f32),
            pltpu.VMEM((seq_rows,) + cache_pairs.shape[2:], bf16),
            pltpu.VMEM(w_output.shape, bf16),
            pltpu.VMEM((seq_rows, w_query.shape[1]), f32),
            pltpu.VMEM(w_exp_gate.shape[1:], bf16),
            pltpu.VMEM(w_exp_up.shape[1:], bf16),
            pltpu.VMEM(w_exp_down.shape[1:], bf16),
            pltpu.VMEM(w_dense_gate.shape, bf16),
            pltpu.VMEM(w_dense_up.shape, bf16),
            pltpu.VMEM(w_dense_down.shape, bf16),
            pltpu.VMEM((n_tp, seq_rows, span), bf16),
            pltpu.VMEM((n_tp, seq_rows, span), bf16),
            pltpu.VMEM((n_tp, n_ep, seq_rows, span), bf16),
            pltpu.VMEM((batch, width), f32),
            pltpu.VMEM((n_sets, slots // n_sets, batch // n_sets), bf16),
            pltpu.VMEM((n_sets, batch // n_sets, slots // n_sets), bf16),
            pltpu.VMEM((n_sets, batch // n_sets, 1), f32),
            pltpu.VMEM((n_sets, n_tp, slots // n_sets, span), bf16),
            pltpu.VMEM((n_sets, n_tp, slots // n_sets, span), bf16),
            pltpu.VMEM((batch, span), f32),
            pltpu.VMEM((n_ep, seq_rows, span), bf16),
            pltpu.VMEM((n_ep, seq_rows, span), bf16),
            dma((11,)),
            dma((seq_rows // 8,)),
            dma((11,)),
            dma, dma,
            dma, dma((n_ep,)),
            dma, dma((n_ep,)), dma((n_ep,)),
            dma((n_sets,)), dma((n_sets,)),
            dma, dma((n_ep,)),
        ],
        compiler_params=pltpu.CompilerParams(
            collective_id=0, has_side_effects=True, vmem_limit_bytes=VMEM_BYTES),
        name="whole_layer",
    )(tokens, attn_gain.reshape(1, width), query_gain.reshape(1, -1), key_gain.reshape(1, -1),
      w_forget.reshape(1, width), forget_bias.reshape(1, 1), lengths.reshape(1, seq_rows),
      ffn_gain.reshape(1, width), expert_ids.T, route_weight.T, shared_gate.reshape(width // 128, 128),
      w_query, w_key.T, w_value.T, cache_cum, cache_pairs, w_output,
      w_exp_gate, w_exp_up, w_exp_down,
      w_dense_gate, w_dense_up, w_dense_down)


def shards(
    tokens,
    attn_gain,
    w_query,
    w_key,
    w_value,
    w_forget,
    forget_bias,
    query_gain,
    key_gain,
    cache_pairs,
    cache_cum,
    lengths,
    w_output,
    ffn_gain,
    expert_ids,
    route_weight,
    w_exp_gate,
    w_exp_up,
    w_exp_down,
    shared_gate,
    w_dense_gate,
    w_dense_up,
    w_dense_down,
):
    return layer_call(
        tokens, attn_gain, w_query, w_key, w_value, w_forget, forget_bias, query_gain, key_gain,
        cache_pairs, cache_cum, lengths, w_output, ffn_gain, expert_ids, route_weight, shared_gate,
        w_exp_gate, w_exp_up, w_exp_down, w_dense_gate, w_dense_up, w_dense_down,
    )


def solution(mesh):
    in_specs = (
        P("ep", None),
        P(),
        P(None, "tp"),
        P(None, "tp"),
        P(None, "tp"),
        P(None, "tp"),
        P("tp"),
        P(),
        P(),
        P("ep", "tp", None, None),
        P("ep", "tp", None),
        P("ep"),
        P("tp", None),
        P(),
        P(),
        P(),
        P("ep", None, "tp"),
        P("ep", None, "tp"),
        P("ep", "tp", None),
        P(),
        P("ep", None),
        P("ep", None),
        P("ep", "tp"),
    )
    out_specs = P("ep", "tp")
    return jax.shard_map(shards, mesh=mesh, in_specs=in_specs, out_specs=out_specs, check_vma=False)
```

```python
import functools

import jax
import jax.numpy as jnp
from jax import lax
from jax.experimental import pallas as pl
from jax.experimental.pallas import tpu as pltpu
from jax.sharding import PartitionSpec as P

EPSILON = 1e-06
MESH = pl.DeviceIdType.MESH
VMEM_BYTES = 56 * 1024 * 1024


def block_sets(n_ep):
    if n_ep == 8:
        return [[0, 1], [2, 3], [4, 5, 6, 7]]
    return [list(range(n_ep))]


def whole_layer(
    n_ep, n_tp, cap,
    tokens_hbm, attn_gain_hbm, query_gain_hbm, key_gain_hbm, forget_hbm, bias_hbm, length_hbm,
    gain_hbm, ids_hbm, route_hbm, shared_hbm,
    wq_hbm, wk_hbm, wv_hbm, cum_hbm, cache_hbm, wo_hbm,
    wg_hbm, wu_hbm, wd_hbm, dg_hbm, du_hbm, dd_hbm,
    out_ref,
    tokens_ref, attn_gain_ref, query_gain_ref, key_gain_ref, forget_ref, bias_ref, length_ref,
    gain_ref, ids_ref, route_ref, shared_ref,
    wq, wkv, cum, cache, wo_ref, mixed,
    wgu, wd, dgu, dd,
    part_out, part_in, gathered, rows_f, pick_ref, place_ref, weight_ref, exp_out, exp_in, total, sum_out, sum_in,
    small_sem, attn_sem, load_sem, part_send, part_recv, ring_send, ring_recv, fan_send, fan_recv,
    exp_send, exp_recv, sum_send, sum_recv,
):
    me = lax.axis_index("ep")
    col = lax.axis_index("tp")
    seq_rows, width = tokens_ref.shape
    span = width // n_tp
    slots = n_ep * cap
    batch = n_ep * seq_rows
    f32, bf16 = jnp.float32, jnp.bfloat16
    head = query_gain_ref.shape[1]
    heads = wq.shape[1] // head
    lanes = 2 * head
    eight = 8
    bunch = eight
    small = [
        pltpu.make_async_copy(src, dst, small_sem.at[i])
        for i, (src, dst) in enumerate((
            (tokens_hbm, tokens_ref), (attn_gain_hbm, attn_gain_ref), (wq_hbm, wq),
            (wk_hbm, wkv.at[pl.ds(0, head)]),
            (forget_hbm, forget_ref), (bias_hbm, bias_ref), (length_hbm, length_ref),
            (query_gain_hbm, query_gain_ref), (key_gain_hbm, key_gain_ref), (cum_hbm.at[:, 0], cum)))
    ]
    small.insert(4, pltpu.make_async_copy(wv_hbm, wkv.at[pl.ds(head, head)], small_sem.at[3]))
    both = pltpu.make_async_copy(wkv, wkv, small_sem.at[3])
    caches = [
        pltpu.make_async_copy(cache_hbm.at[pl.ds(b, bunch), 0], cache.at[pl.ds(b, bunch)], attn_sem.at[b // bunch])
        for b in range(0, seq_rows, bunch)
    ]
    later = [
        pltpu.make_async_copy(src, dst, load_sem.at[i])
        for i, (src, dst) in enumerate((
            (wo_hbm, wo_ref), (gain_hbm, gain_ref), (ids_hbm, ids_ref), (route_hbm, route_ref),
            (shared_hbm, shared_ref), (wg_hbm, wgu.at[pl.ds(0, 1)]), (wd_hbm.at[0], wd),
            (dg_hbm, dgu.at[0]), (dd_hbm, dd)))
    ]
    later.insert(6, pltpu.make_async_copy(wu_hbm, wgu.at[pl.ds(1, 1)], load_sem.at[5]))
    later.insert(9, pltpu.make_async_copy(du_hbm, dgu.at[1], load_sem.at[7]))
    held = [pltpu.make_async_copy(wgu, wgu, load_sem.at[5]), later[7], pltpu.make_async_copy(dgu, dgu, load_sem.at[7]), later[10]]
    for load in small + caches + later[:5]:
        load.start()

    barrier = pltpu.get_barrier_semaphore()
    for k in range(1, n_ep):
        pl.semaphore_signal(barrier, inc=1, device_id={"ep": lax.rem(me + k, n_ep)}, device_id_type=MESH)
    for d in range(1, n_tp):
        pl.semaphore_signal(barrier, inc=1, device_id={"tp": lax.rem(col + d, n_tp)}, device_id_type=MESH)

    def columns(d):
        return pl.ds(pl.multiple_of(lax.rem(col + d, n_tp) * span, span), span)

    def to_tp(src, dst, send, recv, d):
        return pltpu.make_async_remote_copy(
            src_ref=src, dst_ref=dst, send_sem=send, recv_sem=recv,
            device_id={"tp": lax.rem(col + d, n_tp)}, device_id_type=MESH)

    def to_ep(src, dst, send, recv, peer):
        return pltpu.make_async_remote_copy(
            src_ref=src, dst_ref=dst, send_sem=send, recv_sem=recv,
            device_id={"ep": peer}, device_id_type=MESH)

    if n_ep == 8:
        deep, side = me // 2, lax.rem(me, 2)
        low = (deep < 2).astype(jnp.int32)
        inner = low * deep + (1 - low) * (3 - deep)
        line = [inner, 1 - inner, 2, 3]
        line = [low * at + (1 - low) * (3 - at) for at in line]
        away = [line[k // 2] * 2 + (side if k % 2 == 0 else 1 - side) for k in range(n_ep - 1, 0, -1)]
    else:
        away = [lax.rem(me + k, n_ep) for k in range(1, n_ep)]
    rising = [k + (me <= k).astype(jnp.int32) for k in range(n_ep - 1)]
    sets = block_sets(n_ep)

    contract = (((1,), (1,)), ((), ()))

    def iota(shape, axis):
        return lax.broadcasted_iota(jnp.int32, shape, axis).astype(f32)

    def group_of(values, size):
        return jnp.floor((values + 0.5) * (1.0 / size))

    def rms(values, gain):
        return values * lax.rsqrt(jnp.mean(values * values, axis=1, keepdims=True) + EPSILON) * gain

    def rounded(values):
        return values.astype(bf16).astype(f32)

    def half_turn(values):
        return pltpu.roll(values, head, 1)

    left = lax.broadcasted_iota(jnp.int32, (seq_rows, lanes), 1) < head
    small[0].wait()
    small[1].wait()
    token_f = tokens_ref[...].astype(f32)
    normed_one = rms(token_f, attn_gain_ref[...]).astype(bf16)
    small[2].wait()
    query_raw = jnp.dot(normed_one, wq[...], preferred_element_type=f32)
    for load in [both] + small[5:10]:
        load.wait()
    pair_raw = lax.dot_general(normed_one, wkv[...], contract, preferred_element_type=f32)
    gate_in = jnp.sum(normed_one.astype(f32) * forget_ref[...].astype(f32), axis=1, keepdims=True) + bias_ref[...]
    log_gate = jnp.minimum(gate_in, 0.0) - jnp.log(1.0 + jnp.exp(-jnp.abs(gate_in)))
    eye = iota((seq_rows, seq_rows), 0) == iota((seq_rows, seq_rows), 1)
    lengths = jnp.sum(jnp.where(eye, jnp.broadcast_to(length_ref[...].astype(f32), (seq_rows, seq_rows)), 0.0), axis=1, keepdims=True)

    def half_scales(values):
        squares = values * values
        first = jnp.sum(jnp.where(left, squares, 0.0), axis=1, keepdims=True)
        second = jnp.sum(jnp.where(left, 0.0, squares), axis=1, keepdims=True)
        return lax.rsqrt(first / head + EPSILON), lax.rsqrt(second / head + EPSILON)

    gain_twice = jnp.concatenate([query_gain_ref[...]] * 2, axis=1)
    queries = []
    for a in range(heads // 2):
        raw = query_raw[:, lanes * a:lanes * (a + 1)]
        first, second = half_scales(raw)
        query = rounded(raw * jnp.where(left, first, second) * gain_twice)
        turned = half_turn(query)
        queries += [jnp.where(left, query, turned), jnp.where(left, turned, query)]
    key_scale, _ = half_scales(pair_raw)
    key_gain = jnp.concatenate([key_gain_ref[...]] * 2, axis=1)
    key = jnp.where(left, rounded(pair_raw * key_scale * key_gain), 0.0)
    value = rounded(pair_raw)
    value = jnp.where(left, half_turn(value), value)
    multiplier = head ** (-0.5)
    own_scores = [jnp.sum(query * key, axis=1, keepdims=True) * multiplier for query in queries]
    scaled = [query * multiplier for query in queries]
    small[10].wait()
    position = iota(cum.shape, 1)
    now = jnp.sum(jnp.where(position == lengths - 1.0, cum[...], 0.0), axis=1, keepdims=True) + log_gate
    cum[...] = jnp.where(position < lengths, now - cum[...], -1e30)

    row = lax.broadcasted_iota(jnp.int32, (eight, lanes), 0)
    left_eight = lax.broadcasted_iota(jnp.int32, (eight, lanes), 1) < head
    key_at = [row == jnp.where(left_eight, 2 * p, 2 * p + 1) for p in range(eight // 2)]
    value_at = [row == jnp.where(left_eight, 2 * p + 1, 2 * p) for p in range(eight // 2)]

    def score_of(i):
        lines = slice(i * eight, (i + 1) * eight)
        lhs = jnp.concatenate([
            jnp.concatenate([jnp.where(key_at[p], query[lines], 0.0) for query in scaled], axis=0)
            for p in range(eight // 2)], axis=1).astype(bf16)
        keys = jnp.concatenate([cache[i * eight + b, :, 0:head] for b in range(eight)], axis=1)
        return lax.dot_general(lhs, keys, contract, preferred_element_type=f32)

    def attend(i, score):
        lines = slice(i * eight, (i + 1) * eight)
        score = score + jnp.concatenate([cum[lines, :]] * heads, axis=0)
        own = jnp.concatenate([values[lines] for values in own_scores], axis=0)
        peak = jnp.maximum(jnp.max(score, axis=1, keepdims=True), own)
        past = jnp.exp(score - peak)
        own = jnp.exp(own - peak)
        inverse = 1.0 / (jnp.sum(past, axis=1, keepdims=True) + own)
        prob = (past * inverse).astype(bf16)
        own = rounded(own * inverse)
        values = jnp.concatenate([cache[i * eight + (b ^ 1), :, head:2 * head] for b in range(eight)], axis=1)
        wide = jnp.dot(prob, values, preferred_element_type=f32)
        mixes = []
        for h in range(heads):
            here = slice(h * eight, (h + 1) * eight)
            mix = sum(jnp.where(value_at[p], wide[here, lanes * p:lanes * (p + 1)], 0.0) for p in range(eight // 2))
            mixes.append(mix + half_turn(mix) + own[here] * value[lines])
        for a in range(heads // 2):
            mixed[lines, lanes * a:lanes * (a + 1)] = jnp.where(left_eight, mixes[2 * a], mixes[2 * a + 1])

    score = None
    for i in range(seq_rows // eight):
        for load in caches[i * eight // bunch:(i + 1) * eight // bunch]:
            load.wait()
        ahead = score_of(i)
        if score is not None:
            attend(i - 1, score)
        score = ahead
    for load in later[5:]:
        load.start()
    attend(seq_rows // eight - 1, score)
    head_mix = mixed[...].astype(bf16)
    later[0].wait()

    partial = jnp.dot(head_mix, wo_ref[...], preferred_element_type=f32).astype(bf16)
    for j in range(n_tp):
        part_out[j] = partial[:, j * span:(j + 1) * span]
    pl.semaphore_wait(barrier, n_ep + n_tp - 2)
    for d in range(1, n_tp):
        there = lax.rem(col + d, n_tp)
        to_tp(part_out.at[there], part_in.at[col], part_send, part_recv, d).start()
    some = pl.ds(0, n_tp - 1)
    parts = to_tp(part_out.at[some], part_in.at[some], part_send, part_recv, 1)
    token_block = tokens_ref[:, columns(0)].astype(f32)
    part_in[col] = part_out[col]
    parts.wait_recv()
    attn = part_in[0].astype(f32)
    for j in range(1, n_tp):
        attn = attn + part_in[j].astype(f32)
    residual = (token_block + attn).astype(bf16)
    gathered[col, me] = residual

    for peer in away:
        to_ep(gathered.at[col, me], gathered.at[col, me], ring_send, ring_recv.at[me], peer).start()
    if n_tp == 4:
        across = lax.rem(col + 2, 4)
        others = [across, across + 1 - 2 * lax.rem(col, 2), col + 1 - 2 * lax.rem(col, 2)]
    else:
        others = [lax.rem(col + d, n_tp) for d in range(1, n_tp)]

    def fan(slot):
        for other in others:
            pltpu.make_async_remote_copy(
                src_ref=gathered.at[col, slot], dst_ref=gathered.at[col, slot],
                send_sem=fan_send, recv_sem=fan_recv.at[set_of(slot)],
                device_id={"tp": other}, device_id_type=MESH).start()

    def set_of(slot):
        return sum((slot >= chosen[0]).astype(jnp.int32) for chosen in sets) - 1

    def spread(n):
        group = gathered.at[pl.ds(0, n_tp - 1), pl.ds(sets[n][0], len(sets[n]))]
        return pltpu.make_async_remote_copy(
            src_ref=group, dst_ref=group, send_sem=fan_send, recv_sem=fan_recv.at[n],
            device_id={"tp": others[0]}, device_id_type=MESH)

    fan(me)
    for load in later[1:5]:
        load.wait()
    def token_lines(chosen):
        return slice(chosen[0] * seq_rows, (chosen[-1] + 1) * seq_rows)

    def slot_lines(chosen):
        return slice(chosen[0] * cap, (chosen[-1] + 1) * cap)

    expert = me
    hit = jnp.zeros((1, batch), f32)
    weight_row = jnp.zeros((1, batch), f32)
    for k in range(ids_ref.shape[0]):
        same = ids_ref[k:k + 1, :] == expert
        hit = hit + jnp.where(same, 1.0, 0.0)
        weight_row = weight_row + jnp.where(same, route_ref[k:k + 1, :], 0.0)
    row_at = iota((batch, batch), 0)
    col_at = iota((batch, batch), 1)
    hits = jnp.broadcast_to(hit, (8, batch)).astype(bf16)
    hit = hits[0:1].astype(f32)
    before = (row_at <= col_at) & (row_at >= group_of(col_at, seq_rows) * seq_rows)
    rank = jnp.dot(hits, before.astype(f32).astype(bf16), preferred_element_type=f32)[0:1]
    slot_of = jnp.where((hit > 0.5) & (rank < cap + 0.5), group_of(iota((1, batch), 1), seq_rows) * cap + rank - 1.0, -1.0)
    for n, chosen in enumerate(sets):
        lines, places = token_lines(chosen), slot_lines(chosen)
        here = slot_of[:, lines]
        size = len(chosen) * cap, len(chosen) * seq_rows
        pick = jnp.where(iota(size, 0) + chosen[0] * cap == here, 1.0, 0.0)
        pick_ref[n, 0:size[0], 0:size[1]] = pick.astype(bf16)
        place_ref[n, 0:size[1], 0:size[0]] = pick.T.astype(bf16)
        weight_ref[lines, :] = jnp.sum((pick * weight_row[:, lines]).T, axis=1, keepdims=True)
    shared_tiles = shared_ref[...].astype(f32)
    shared = jnp.concatenate([shared_tiles[i:i + 1] for i in range(width // 128)], axis=1)

    def lines_of(slot):
        return slice(slot * seq_rows, (slot + 1) * seq_rows)

    def normalize(k):
        blocks = [gathered[t, k].astype(f32) for t in range(n_tp)]
        squares = sum(jnp.sum(b * b, axis=1, keepdims=True) for b in blocks)
        scale = lax.rsqrt(squares / width + EPSILON)
        for t in range(n_tp):
            rows_f[lines_of(k), t * span:(t + 1) * span] = (
                blocks[t] * scale * gain_ref[:, t * span:(t + 1) * span])

    def expert_part(n, chosen):
        rows = rows_f[token_lines(chosen), :].astype(bf16)
        pick = pick_ref[n, 0:len(chosen) * cap, 0:len(chosen) * seq_rows]
        picked = jnp.dot(pick, rows, preferred_element_type=f32).astype(bf16)
        gate = jnp.dot(picked, wgu[0], preferred_element_type=f32)
        up = jnp.dot(picked, wgu[1], preferred_element_type=f32)
        hidden = (gate / (1.0 + jnp.exp(-gate)) * up).astype(bf16)
        down = jnp.dot(hidden, wd[...], preferred_element_type=f32).astype(bf16)
        places = slot_lines(chosen)
        for j in range(n_tp):
            exp_out[j, places, :] = down[:, j * span:(j + 1) * span]
        part = pl.ds(chosen[0] * cap, len(chosen) * cap)
        for d in sorted(range(1, n_tp), key=lambda d: d != 2):
            there = lax.rem(col + d, n_tp)
            to_tp(exp_out.at[there, part], exp_in.at[col, part], exp_send.at[n], exp_recv.at[n], d).start()
        exp_in[col, places, :] = exp_out[col, places, :]

    def moves(n):
        there = exp_in.at[pl.ds(0, n_tp - 1), pl.ds(sets[n][0] * cap, len(sets[n]) * cap)]
        return to_tp(there, there, exp_send.at[n], exp_recv.at[n], 1)

    def dense(rows):
        rows = rows.astype(bf16)
        gate = lax.dot_general(rows, dgu[0], contract, preferred_element_type=f32)
        up = lax.dot_general(rows, dgu[1], contract, preferred_element_type=f32)
        hidden = (gate / (1.0 + jnp.exp(-gate)) * up).astype(bf16)
        mix = jnp.sum(rows.astype(f32) * shared, axis=1, keepdims=True)
        mix = 1.0 / (1.0 + jnp.exp(-mix))
        return mix * jnp.dot(hidden, dd[...], preferred_element_type=f32)

    def finish(n, chosen):
        moves(n).wait_recv()
        places, lines = slot_lines(chosen), token_lines(chosen)
        rows = exp_in[0, places, :].astype(f32)
        for j in range(1, n_tp):
            rows = rows + exp_in[j, places, :].astype(f32)
        place = place_ref[n, 0:len(chosen) * seq_rows, 0:len(chosen) * cap]
        placed = jnp.dot(place, rows.astype(bf16), preferred_element_type=f32) * weight_ref[lines, :]
        total[lines, :] = total[lines, :] + placed
        for slot in chosen:
            sum_out[slot] = total[lines_of(slot), :].astype(bf16)
        for slot in (chosen if 2 * n < len(sets) else reversed(chosen)):
            @pl.when(slot != me)
            def _():
                to_ep(sum_out.at[slot], sum_in.at[me], sum_send, sum_recv, slot).start()

    for slot in rising:
        to_ep(gathered.at[col, slot], gathered.at[col, slot], ring_send, ring_recv.at[slot], slot).wait_recv()
        fan(slot)
    for load in held:
        load.wait()
    for n, chosen in enumerate(sets):
        spread(n).wait_recv()
        for k in chosen:
            normalize(k)
        expert_part(n, chosen)
    step = seq_rows * 8 if n_ep % 8 == 0 else batch
    if step == batch:
        total[...] = dense(rows_f[...])
    else:
        @pl.loop(0, batch // step)
        def _(i):
            at = pl.multiple_of(i * step, step)
            total[pl.ds(at, step), :] = dense(rows_f[pl.ds(at, step), :])
    for n, chosen in enumerate(sets):
        finish(n, chosen)
    most = pl.ds(0, n_ep - 1)
    result = residual.astype(f32) + total[pl.ds(pl.multiple_of(me * seq_rows, 8), seq_rows), :]
    sums = to_ep(sum_in.at[most], sum_in.at[most], sum_send, sum_recv, away[0])
    sums.wait_recv()
    sum_in[me] = jnp.zeros_like(sum_in[me])
    for slot in range(n_ep):
        result = result + sum_in[slot].astype(f32)
    out_ref[...] = result.astype(bf16)
    parts.wait_send()
    to_ep(gathered.at[0, most], gathered.at[0, most], ring_send, ring_recv.at[0], away[0]).wait_send()
    for n in range(len(sets)):
        spread(n).wait_send()
    for n in range(len(sets)):
        moves(n).wait_send()
    sums.wait_send()


def layer_call(tokens, attn_gain, w_query, w_key, w_value, w_forget, forget_bias, query_gain, key_gain,
              cache_pairs, cache_cum, lengths, w_output, ffn_gain, expert_ids, route_weight, shared_gate,
              w_exp_gate, w_exp_up, w_exp_down, w_dense_gate, w_dense_up, w_dense_down):
    n_ep, n_tp = lax.axis_size("ep"), lax.axis_size("tp")
    seq_rows, width = tokens.shape
    cap = max(2, min(seq_rows, 128 // n_ep))
    sets = block_sets(n_ep)
    n_sets, most = len(sets), max(len(chosen) for chosen in sets)
    span = width // n_tp
    slots, batch = n_ep * cap, n_ep * seq_rows
    bf16, f32 = jnp.bfloat16, jnp.float32
    vmem = pl.BlockSpec(memory_space=pltpu.VMEM)
    hbm = pl.BlockSpec(memory_space=pltpu.HBM)
    dma = pltpu.SemaphoreType.DMA
    return pl.pallas_call(
        functools.partial(whole_layer, n_ep, n_tp, cap),
        out_shape=pltpu.VMEM((seq_rows, span), bf16),
        in_specs=[hbm] * 23,
        out_specs=vmem,
        scratch_shapes=[
            pltpu.VMEM(tokens.shape, bf16),
            pltpu.VMEM((1, width), f32),
            pltpu.VMEM((1, query_gain.shape[0]), f32),
            pltpu.VMEM((1, key_gain.shape[0]), f32),
            pltpu.VMEM((1, width), bf16),
            pltpu.VMEM((1, 1), f32),
            pltpu.VMEM((1, seq_rows), jnp.int32),
            pltpu.VMEM((1, width), f32),
            pltpu.VMEM(expert_ids.shape[::-1], jnp.int32),
            pltpu.VMEM(route_weight.shape[::-1], f32),
            pltpu.VMEM((width // 128, 128), bf16),
            pltpu.VMEM(w_query.shape, bf16),
            pltpu.VMEM((2 * w_key.shape[1], width), bf16),
            pltpu.VMEM((seq_rows, cache_cum.shape[2]), f32),
            pltpu.VMEM((seq_rows,) + cache_pairs.shape[2:], bf16),
            pltpu.VMEM(w_output.shape, bf16),
            pltpu.VMEM((seq_rows, w_query.shape[1]), f32),
            pltpu.VMEM((2,) + w_exp_gate.shape[1:], bf16),
            pltpu.VMEM(w_exp_down.shape[1:], bf16),
            pltpu.VMEM((2,) + w_dense_gate.shape, bf16),
            pltpu.VMEM(w_dense_down.shape, bf16),
            pltpu.VMEM((n_tp, seq_rows, span), bf16),
            pltpu.VMEM((n_tp, seq_rows, span), bf16),
            pltpu.VMEM((n_tp, n_ep, seq_rows, span), bf16),
            pltpu.VMEM((batch, width), f32),
            pltpu.VMEM((n_sets, most * cap, most * seq_rows), bf16),
            pltpu.VMEM((n_sets, most * seq_rows, most * cap), bf16),
            pltpu.VMEM((batch, 1), f32),
            pltpu.VMEM((n_tp, slots, span), bf16),
            pltpu.VMEM((n_tp, slots, span), bf16),
            pltpu.VMEM((batch, span), f32),
            pltpu.VMEM((n_ep, seq_rows, span), bf16),
            pltpu.VMEM((n_ep, seq_rows, span), bf16),
            dma((10,)),
            dma((seq_rows // 8,)),
            dma((9,)),
            dma, dma,
            dma, dma((n_ep,)),
            dma, dma((n_sets,)),
            dma((n_sets,)), dma((n_sets,)),
            dma, dma,
        ],
        compiler_params=pltpu.CompilerParams(
            collective_id=0, has_side_effects=True, vmem_limit_bytes=VMEM_BYTES),
        name="whole_layer",
    )(tokens, attn_gain.reshape(1, width), query_gain.reshape(1, -1), key_gain.reshape(1, -1),
      w_forget.reshape(1, width), forget_bias.reshape(1, 1), lengths.reshape(1, seq_rows),
      ffn_gain.reshape(1, width), expert_ids.T, route_weight.T, shared_gate.reshape(width // 128, 128),
      w_query, w_key.T, w_value.T, cache_cum, cache_pairs, w_output,
      w_exp_gate, w_exp_up, w_exp_down,
      w_dense_gate, w_dense_up, w_dense_down)


def shards(
    tokens,
    attn_gain,
    w_query,
    w_key,
    w_value,
    w_forget,
    forget_bias,
    query_gain,
    key_gain,
    cache_pairs,
    cache_cum,
    lengths,
    w_output,
    ffn_gain,
    expert_ids,
    route_weight,
    w_exp_gate,
    w_exp_up,
    w_exp_down,
    shared_gate,
    w_dense_gate,
    w_dense_up,
    w_dense_down,
):
    return layer_call(
        tokens, attn_gain, w_query, w_key, w_value, w_forget, forget_bias, query_gain, key_gain,
        cache_pairs, cache_cum, lengths, w_output, ffn_gain, expert_ids, route_weight, shared_gate,
        w_exp_gate, w_exp_up, w_exp_down, w_dense_gate, w_dense_up, w_dense_down,
    )


def solution(mesh):
    in_specs = (
        P("ep", None),
        P(),
        P(None, "tp"),
        P(None, "tp"),
        P(None, "tp"),
        P(None, "tp"),
        P("tp"),
        P(),
        P(),
        P("ep", "tp", None, None),
        P("ep", "tp", None),
        P("ep"),
        P("tp", None),
        P(),
        P(),
        P(),
        P("ep", None, "tp"),
        P("ep", None, "tp"),
        P("ep", "tp", None),
        P(),
        P("ep", None),
        P("ep", None),
        P("ep", "tp"),
    )
    out_specs = P("ep", "tp")
    return jax.shard_map(shards, mesh=mesh, in_specs=in_specs, out_specs=out_specs, check_vma=False)
```

```python
import functools

import jax
import jax.numpy as jnp
from jax import lax
from jax.experimental import pallas as pl
from jax.experimental.pallas import tpu as pltpu
from jax.sharding import PartitionSpec as P

EPSILON = 1e-06
MESH = pl.DeviceIdType.MESH
VMEM_BYTES = 56 * 1024 * 1024


def block_sets(n_ep):
    if n_ep == 8:
        return [[0], [1, 2, 3], [4, 5, 6, 7]]
    return [list(range(n_ep))]


def whole_layer(
    n_ep, n_tp, cap,
    tokens_hbm, attn_gain_hbm, query_gain_hbm, key_gain_hbm, forget_hbm, bias_hbm, length_hbm,
    gain_hbm, ids_hbm, route_hbm, shared_hbm,
    wq_hbm, wk_hbm, wv_hbm, cum_hbm, cache_hbm, wo_hbm,
    wg_hbm, wu_hbm, wd_hbm, dg_hbm, du_hbm, dd_hbm,
    out_ref,
    tokens_ref, attn_gain_ref, query_gain_ref, key_gain_ref, forget_ref, bias_ref, length_ref,
    gain_ref, ids_ref, route_ref, shared_ref,
    wq, wkv, cum, cache, wo_ref, mixed,
    wgu, wd, dgu, dd,
    part_out, part_in, gathered, rows_f, pick_ref, place_ref, weight_ref, exp_out, exp_in, total, sum_out, sum_in,
    small_sem, attn_sem, load_sem, part_send, part_recv, ring_send, ring_recv, fan_send, fan_recv,
    exp_send, exp_recv, sum_send, sum_recv,
):
    me = lax.axis_index("ep")
    col = lax.axis_index("tp")
    seq_rows, width = tokens_ref.shape
    span = width // n_tp
    slots = n_ep * cap
    batch = n_ep * seq_rows
    f32, bf16 = jnp.float32, jnp.bfloat16
    head = query_gain_ref.shape[1]
    heads = wq.shape[1] // head
    lanes = 2 * head
    eight = 8
    bunch = eight
    small = [
        pltpu.make_async_copy(src, dst, small_sem.at[i])
        for i, (src, dst) in enumerate((
            (tokens_hbm, tokens_ref), (attn_gain_hbm, attn_gain_ref), (wq_hbm, wq),
            (wk_hbm, wkv.at[pl.ds(0, head)]),
            (forget_hbm, forget_ref), (bias_hbm, bias_ref), (length_hbm, length_ref),
            (query_gain_hbm, query_gain_ref), (key_gain_hbm, key_gain_ref), (cum_hbm.at[:, 0], cum)))
    ]
    small.insert(4, pltpu.make_async_copy(wv_hbm, wkv.at[pl.ds(head, head)], small_sem.at[3]))
    both = pltpu.make_async_copy(wkv, wkv, small_sem.at[3])
    caches = [
        pltpu.make_async_copy(cache_hbm.at[pl.ds(b, bunch), 0], cache.at[pl.ds(b, bunch)], attn_sem.at[b // bunch])
        for b in range(0, seq_rows, bunch)
    ]
    later = [
        pltpu.make_async_copy(src, dst, load_sem.at[i])
        for i, (src, dst) in enumerate((
            (wo_hbm, wo_ref), (gain_hbm, gain_ref), (ids_hbm, ids_ref), (route_hbm, route_ref),
            (shared_hbm, shared_ref), (wg_hbm, wgu.at[pl.ds(0, 1)]), (wd_hbm.at[0], wd),
            (dg_hbm, dgu.at[0]), (dd_hbm, dd)))
    ]
    later.insert(6, pltpu.make_async_copy(wu_hbm, wgu.at[pl.ds(1, 1)], load_sem.at[5]))
    later.insert(9, pltpu.make_async_copy(du_hbm, dgu.at[1], load_sem.at[7]))
    held = [pltpu.make_async_copy(wgu, wgu, load_sem.at[5]), later[7], pltpu.make_async_copy(dgu, dgu, load_sem.at[7]), later[10]]
    for load in small + caches + later[:5]:
        load.start()

    barrier = pltpu.get_barrier_semaphore()
    for k in range(1, n_ep):
        pl.semaphore_signal(barrier, inc=1, device_id={"ep": lax.rem(me + k, n_ep)}, device_id_type=MESH)
    for d in range(1, n_tp):
        pl.semaphore_signal(barrier, inc=1, device_id={"tp": lax.rem(col + d, n_tp)}, device_id_type=MESH)

    def columns(d):
        return pl.ds(pl.multiple_of(lax.rem(col + d, n_tp) * span, span), span)

    def to_tp(src, dst, send, recv, d):
        return pltpu.make_async_remote_copy(
            src_ref=src, dst_ref=dst, send_sem=send, recv_sem=recv,
            device_id={"tp": lax.rem(col + d, n_tp)}, device_id_type=MESH)

    def to_ep(src, dst, send, recv, peer):
        return pltpu.make_async_remote_copy(
            src_ref=src, dst_ref=dst, send_sem=send, recv_sem=recv,
            device_id={"ep": peer}, device_id_type=MESH)

    if n_ep == 8:
        deep, side = me // 2, lax.rem(me, 2)
        low = (deep < 2).astype(jnp.int32)
        inner = low * deep + (1 - low) * (3 - deep)
        line = [inner, 1 - inner, 2, 3]
        line = [low * at + (1 - low) * (3 - at) for at in line]
        away = [line[k // 2] * 2 + (side if k % 2 == 0 else 1 - side) for k in range(n_ep - 1, 0, -1)]
    else:
        away = [lax.rem(me + k, n_ep) for k in range(1, n_ep)]
    rising = [k + (me <= k).astype(jnp.int32) for k in range(n_ep - 1)]
    sets = block_sets(n_ep)

    contract = (((1,), (1,)), ((), ()))

    def iota(shape, axis):
        return lax.broadcasted_iota(jnp.int32, shape, axis).astype(f32)

    def group_of(values, size):
        return jnp.floor((values + 0.5) * (1.0 / size))

    def rms(values, gain):
        return values * lax.rsqrt(jnp.mean(values * values, axis=1, keepdims=True) + EPSILON) * gain

    def rounded(values):
        return values.astype(bf16).astype(f32)

    def half_turn(values):
        return pltpu.roll(values, head, 1)

    left = lax.broadcasted_iota(jnp.int32, (seq_rows, lanes), 1) < head
    small[0].wait()
    small[1].wait()
    token_f = tokens_ref[...].astype(f32)
    normed_one = rms(token_f, attn_gain_ref[...]).astype(bf16)
    small[2].wait()
    query_raw = jnp.dot(normed_one, wq[...], preferred_element_type=f32)
    for load in [both] + small[5:10]:
        load.wait()
    pair_raw = lax.dot_general(normed_one, wkv[...], contract, preferred_element_type=f32)
    gate_in = jnp.sum(normed_one.astype(f32) * forget_ref[...].astype(f32), axis=1, keepdims=True) + bias_ref[...]
    log_gate = jnp.minimum(gate_in, 0.0) - jnp.log(1.0 + jnp.exp(-jnp.abs(gate_in)))
    eye = iota((seq_rows, seq_rows), 0) == iota((seq_rows, seq_rows), 1)
    lengths = jnp.sum(jnp.where(eye, jnp.broadcast_to(length_ref[...].astype(f32), (seq_rows, seq_rows)), 0.0), axis=1, keepdims=True)

    def half_scales(values):
        squares = values * values
        first = jnp.sum(jnp.where(left, squares, 0.0), axis=1, keepdims=True)
        second = jnp.sum(jnp.where(left, 0.0, squares), axis=1, keepdims=True)
        return lax.rsqrt(first / head + EPSILON), lax.rsqrt(second / head + EPSILON)

    gain_twice = jnp.concatenate([query_gain_ref[...]] * 2, axis=1)
    queries = []
    for a in range(heads // 2):
        raw = query_raw[:, lanes * a:lanes * (a + 1)]
        first, second = half_scales(raw)
        query = rounded(raw * jnp.where(left, first, second) * gain_twice)
        turned = half_turn(query)
        queries += [jnp.where(left, query, turned), jnp.where(left, turned, query)]
    key_scale, _ = half_scales(pair_raw)
    key_gain = jnp.concatenate([key_gain_ref[...]] * 2, axis=1)
    key = jnp.where(left, rounded(pair_raw * key_scale * key_gain), 0.0)
    value = rounded(pair_raw)
    value = jnp.where(left, half_turn(value), value)
    multiplier = head ** (-0.5)
    own_scores = [jnp.sum(query * key, axis=1, keepdims=True) * multiplier for query in queries]
    scaled = [query * multiplier for query in queries]
    small[10].wait()
    position = iota(cum.shape, 1)
    now = jnp.sum(jnp.where(position == lengths - 1.0, cum[...], 0.0), axis=1, keepdims=True) + log_gate
    cum[...] = jnp.where(position < lengths, now - cum[...], -1e30)

    row = lax.broadcasted_iota(jnp.int32, (eight, lanes), 0)
    left_eight = lax.broadcasted_iota(jnp.int32, (eight, lanes), 1) < head
    key_at = [row == jnp.where(left_eight, 2 * p, 2 * p + 1) for p in range(eight // 2)]
    value_at = [row == jnp.where(left_eight, 2 * p + 1, 2 * p) for p in range(eight // 2)]

    def score_of(i):
        lines = slice(i * eight, (i + 1) * eight)
        lhs = jnp.concatenate([
            jnp.concatenate([jnp.where(key_at[p], query[lines], 0.0) for query in scaled], axis=0)
            for p in range(eight // 2)], axis=1).astype(bf16)
        keys = jnp.concatenate([cache[i * eight + b, :, 0:head] for b in range(eight)], axis=1)
        return lax.dot_general(lhs, keys, contract, preferred_element_type=f32)

    def attend(i, score):
        lines = slice(i * eight, (i + 1) * eight)
        score = score + jnp.concatenate([cum[lines, :]] * heads, axis=0)
        own = jnp.concatenate([values[lines] for values in own_scores], axis=0)
        peak = jnp.maximum(jnp.max(score, axis=1, keepdims=True), own)
        past = jnp.exp(score - peak)
        own = jnp.exp(own - peak)
        inverse = 1.0 / (jnp.sum(past, axis=1, keepdims=True) + own)
        prob = (past * inverse).astype(bf16)
        own = rounded(own * inverse)
        return prob, own

    def gather_values(i, prob, own):
        lines = slice(i * eight, (i + 1) * eight)
        values = jnp.concatenate([cache[i * eight + (b ^ 1), :, head:2 * head] for b in range(eight)], axis=1)
        wide = jnp.dot(prob, values, preferred_element_type=f32)
        mixes = []
        for h in range(heads):
            here = slice(h * eight, (h + 1) * eight)
            mix = sum(jnp.where(value_at[p], wide[here, lanes * p:lanes * (p + 1)], 0.0) for p in range(eight // 2))
            mixes.append(mix + half_turn(mix) + own[here] * value[lines])
        for a in range(heads // 2):
            mixed[lines, lanes * a:lanes * (a + 1)] = jnp.where(left_eight, mixes[2 * a], mixes[2 * a + 1])

    count = seq_rows // eight
    score, prob = {}, {}
    for i in range(count):
        for load in caches[i * eight // bunch:(i + 1) * eight // bunch]:
            load.wait()
        if i > 0:
            prob[i - 1] = attend(i - 1, score[i - 1])
        score[i] = score_of(i)
        if i > 1:
            gather_values(i - 2, *prob[i - 2])
    prob[count - 1] = attend(count - 1, score[count - 1])
    for i in range(max(count - 2, 0), count):
        gather_values(i, *prob[i])
    for load in later[5:]:
        load.start()
    head_mix = mixed[...].astype(bf16)
    later[0].wait()

    partial = jnp.dot(head_mix, wo_ref[...], preferred_element_type=f32).astype(bf16)
    for j in range(n_tp):
        part_out[j] = partial[:, j * span:(j + 1) * span]
    pl.semaphore_wait(barrier, n_ep + n_tp - 2)
    for d in range(1, n_tp):
        there = lax.rem(col + d, n_tp)
        to_tp(part_out.at[there], part_in.at[col], part_send, part_recv, d).start()
    some = pl.ds(0, n_tp - 1)
    parts = to_tp(part_out.at[some], part_in.at[some], part_send, part_recv, 1)
    token_block = tokens_ref[:, columns(0)].astype(f32)
    part_in[col] = part_out[col]
    parts.wait_recv()
    attn = part_in[0].astype(f32)
    for j in range(1, n_tp):
        attn = attn + part_in[j].astype(f32)
    residual = (token_block + attn).astype(bf16)
    gathered[col, me] = residual

    for peer in away:
        to_ep(gathered.at[col, me], gathered.at[col, me], ring_send, ring_recv.at[me], peer).start()
    if n_tp == 4:
        across = lax.rem(col + 2, 4)
        others = [across, across + 1 - 2 * lax.rem(col, 2), col + 1 - 2 * lax.rem(col, 2)]
    else:
        others = [lax.rem(col + d, n_tp) for d in range(1, n_tp)]

    def fan(slot):
        for other in others:
            pltpu.make_async_remote_copy(
                src_ref=gathered.at[col, slot], dst_ref=gathered.at[col, slot],
                send_sem=fan_send, recv_sem=fan_recv.at[set_of(slot)],
                device_id={"tp": other}, device_id_type=MESH).start()

    def set_of(slot):
        return sum((slot >= chosen[0]).astype(jnp.int32) for chosen in sets) - 1

    def spread(n):
        group = gathered.at[pl.ds(0, n_tp - 1), pl.ds(sets[n][0], len(sets[n]))]
        return pltpu.make_async_remote_copy(
            src_ref=group, dst_ref=group, send_sem=fan_send, recv_sem=fan_recv.at[n],
            device_id={"tp": others[0]}, device_id_type=MESH)

    fan(me)
    for load in later[1:5]:
        load.wait()
    def token_lines(chosen):
        return slice(chosen[0] * seq_rows, (chosen[-1] + 1) * seq_rows)

    def slot_lines(chosen):
        return slice(chosen[0] * cap, (chosen[-1] + 1) * cap)

    expert = me
    hit = jnp.zeros((1, batch), f32)
    weight_row = jnp.zeros((1, batch), f32)
    for k in range(ids_ref.shape[0]):
        same = ids_ref[k:k + 1, :] == expert
        hit = hit + jnp.where(same, 1.0, 0.0)
        weight_row = weight_row + jnp.where(same, route_ref[k:k + 1, :], 0.0)
    row_at = iota((batch, batch), 0)
    col_at = iota((batch, batch), 1)
    hits = jnp.broadcast_to(hit, (8, batch)).astype(bf16)
    hit = hits[0:1].astype(f32)
    before = (row_at <= col_at) & (row_at >= group_of(col_at, seq_rows) * seq_rows)
    rank = jnp.dot(hits, before.astype(f32).astype(bf16), preferred_element_type=f32)[0:1]
    slot_of = jnp.where((hit > 0.5) & (rank < cap + 0.5), group_of(iota((1, batch), 1), seq_rows) * cap + rank - 1.0, -1.0)
    for n, chosen in enumerate(sets):
        lines, places = token_lines(chosen), slot_lines(chosen)
        here = slot_of[:, lines]
        size = len(chosen) * cap, len(chosen) * seq_rows
        pick = jnp.where(iota(size, 0) + chosen[0] * cap == here, 1.0, 0.0)
        pick_ref[n, 0:size[0], 0:size[1]] = pick.astype(bf16)
        place_ref[n, 0:size[1], 0:size[0]] = pick.T.astype(bf16)
        weight_ref[lines, :] = jnp.sum((pick * weight_row[:, lines]).T, axis=1, keepdims=True)
    shared_tiles = shared_ref[...].astype(f32)
    shared = jnp.concatenate([shared_tiles[i:i + 1] for i in range(width // 128)], axis=1)

    def lines_of(slot):
        return slice(slot * seq_rows, (slot + 1) * seq_rows)

    def normalize(k):
        blocks = [gathered[t, k].astype(f32) for t in range(n_tp)]
        squares = sum(jnp.sum(b * b, axis=1, keepdims=True) for b in blocks)
        scale = lax.rsqrt(squares / width + EPSILON)
        for t in range(n_tp):
            rows_f[lines_of(k), t * span:(t + 1) * span] = (
                blocks[t] * scale * gain_ref[:, t * span:(t + 1) * span])

    def prepare(n):
        chosen = sets[n]
        for k in chosen:
            normalize(k)
        rows = rows_f[token_lines(chosen), :].astype(bf16)
        pick = pick_ref[n, 0:len(chosen) * cap, 0:len(chosen) * seq_rows]
        return jnp.dot(pick, rows, preferred_element_type=f32).astype(bf16)

    def hidden_of(picked):
        gate = jnp.dot(picked, wgu[0], preferred_element_type=f32)
        up = jnp.dot(picked, wgu[1], preferred_element_type=f32)
        return (gate / (1.0 + jnp.exp(-gate)) * up).astype(bf16)

    def down_of(hidden):
        return jnp.dot(hidden, wd[...], preferred_element_type=f32).astype(bf16)

    def send_moves(n, down):
        chosen = sets[n]
        places = slot_lines(chosen)
        for j in range(n_tp):
            exp_out[j, places, :] = down[:, j * span:(j + 1) * span]
        part = pl.ds(chosen[0] * cap, len(chosen) * cap)
        for d in sorted(range(1, n_tp), key=lambda d: d != 2):
            there = lax.rem(col + d, n_tp)
            to_tp(exp_out.at[there, part], exp_in.at[col, part], exp_send.at[n], exp_recv.at[n], d).start()
        exp_in[col, places, :] = exp_out[col, places, :]

    def moves(n):
        there = exp_in.at[pl.ds(0, n_tp - 1), pl.ds(sets[n][0] * cap, len(sets[n]) * cap)]
        return to_tp(there, there, exp_send.at[n], exp_recv.at[n], 1)

    def dense(rows):
        rows = rows.astype(bf16)
        gate = lax.dot_general(rows, dgu[0], contract, preferred_element_type=f32)
        up = lax.dot_general(rows, dgu[1], contract, preferred_element_type=f32)
        hidden = (gate / (1.0 + jnp.exp(-gate)) * up).astype(bf16)
        mix = jnp.sum(rows.astype(f32) * shared, axis=1, keepdims=True)
        mix = 1.0 / (1.0 + jnp.exp(-mix))
        return mix * jnp.dot(hidden, dd[...], preferred_element_type=f32)

    def finish(n, chosen):
        moves(n).wait_recv()
        places, lines = slot_lines(chosen), token_lines(chosen)
        rows = exp_in[0, places, :].astype(f32)
        for j in range(1, n_tp):
            rows = rows + exp_in[j, places, :].astype(f32)
        place = place_ref[n, 0:len(chosen) * seq_rows, 0:len(chosen) * cap]
        placed = jnp.dot(place, rows.astype(bf16), preferred_element_type=f32) * weight_ref[lines, :]
        total[lines, :] = total[lines, :] + placed
        for slot in chosen:
            sum_out[slot] = total[lines_of(slot), :].astype(bf16)
        for slot in (chosen if 2 * n < len(sets) else reversed(chosen)):
            @pl.when(slot != me)
            def _():
                to_ep(sum_out.at[slot], sum_in.at[me], sum_send, sum_recv, slot).start()

    for slot in rising:
        to_ep(gathered.at[col, slot], gathered.at[col, slot], ring_send, ring_recv.at[slot], slot).wait_recv()
        fan(slot)
    for load in held:
        load.wait()
    spread(0).wait_recv()
    picked = prepare(0)
    for n in range(len(sets)):
        hidden = hidden_of(picked)
        if n + 1 < len(sets):
            spread(n + 1).wait_recv()
        down = down_of(hidden)
        if n + 1 < len(sets):
            picked = prepare(n + 1)
        send_moves(n, down)
    step = seq_rows * 8 if n_ep % 8 == 0 else batch
    if step == batch:
        total[...] = dense(rows_f[...])
    else:
        @pl.loop(0, batch // step)
        def _(i):
            at = pl.multiple_of(i * step, step)
            total[pl.ds(at, step), :] = dense(rows_f[pl.ds(at, step), :])
    for n, chosen in enumerate(sets):
        finish(n, chosen)
    most = pl.ds(0, n_ep - 1)
    result = residual.astype(f32) + total[pl.ds(pl.multiple_of(me * seq_rows, 8), seq_rows), :]
    sums = to_ep(sum_in.at[most], sum_in.at[most], sum_send, sum_recv, away[0])
    sums.wait_recv()
    sum_in[me] = jnp.zeros_like(sum_in[me])
    for slot in range(n_ep):
        result = result + sum_in[slot].astype(f32)
    out_ref[...] = result.astype(bf16)
    parts.wait_send()
    to_ep(gathered.at[0, most], gathered.at[0, most], ring_send, ring_recv.at[0], away[0]).wait_send()
    for n in range(len(sets)):
        spread(n).wait_send()
    for n in range(len(sets)):
        moves(n).wait_send()
    sums.wait_send()


def layer_call(tokens, attn_gain, w_query, w_key, w_value, w_forget, forget_bias, query_gain, key_gain,
              cache_pairs, cache_cum, lengths, w_output, ffn_gain, expert_ids, route_weight, shared_gate,
              w_exp_gate, w_exp_up, w_exp_down, w_dense_gate, w_dense_up, w_dense_down):
    n_ep, n_tp = lax.axis_size("ep"), lax.axis_size("tp")
    seq_rows, width = tokens.shape
    cap = max(2, min(seq_rows, 128 // n_ep))
    sets = block_sets(n_ep)
    n_sets, most = len(sets), max(len(chosen) for chosen in sets)
    span = width // n_tp
    slots, batch = n_ep * cap, n_ep * seq_rows
    bf16, f32 = jnp.bfloat16, jnp.float32
    vmem = pl.BlockSpec(memory_space=pltpu.VMEM)
    hbm = pl.BlockSpec(memory_space=pltpu.HBM)
    dma = pltpu.SemaphoreType.DMA
    return pl.pallas_call(
        functools.partial(whole_layer, n_ep, n_tp, cap),
        out_shape=pltpu.VMEM((seq_rows, span), bf16),
        in_specs=[hbm] * 23,
        out_specs=vmem,
        scratch_shapes=[
            pltpu.VMEM(tokens.shape, bf16),
            pltpu.VMEM((1, width), f32),
            pltpu.VMEM((1, query_gain.shape[0]), f32),
            pltpu.VMEM((1, key_gain.shape[0]), f32),
            pltpu.VMEM((1, width), bf16),
            pltpu.VMEM((1, 1), f32),
            pltpu.VMEM((1, seq_rows), jnp.int32),
            pltpu.VMEM((1, width), f32),
            pltpu.VMEM(expert_ids.shape[::-1], jnp.int32),
            pltpu.VMEM(route_weight.shape[::-1], f32),
            pltpu.VMEM((width // 128, 128), bf16),
            pltpu.VMEM(w_query.shape, bf16),
            pltpu.VMEM((2 * w_key.shape[1], width), bf16),
            pltpu.VMEM((seq_rows, cache_cum.shape[2]), f32),
            pltpu.VMEM((seq_rows,) + cache_pairs.shape[2:], bf16),
            pltpu.VMEM(w_output.shape, bf16),
            pltpu.VMEM((seq_rows, w_query.shape[1]), f32),
            pltpu.VMEM((2,) + w_exp_gate.shape[1:], bf16),
            pltpu.VMEM(w_exp_down.shape[1:], bf16),
            pltpu.VMEM((2,) + w_dense_gate.shape, bf16),
            pltpu.VMEM(w_dense_down.shape, bf16),
            pltpu.VMEM((n_tp, seq_rows, span), bf16),
            pltpu.VMEM((n_tp, seq_rows, span), bf16),
            pltpu.VMEM((n_tp, n_ep, seq_rows, span), bf16),
            pltpu.VMEM((batch, width), f32),
            pltpu.VMEM((n_sets, most * cap, most * seq_rows), bf16),
            pltpu.VMEM((n_sets, most * seq_rows, most * cap), bf16),
            pltpu.VMEM((batch, 1), f32),
            pltpu.VMEM((n_tp, slots, span), bf16),
            pltpu.VMEM((n_tp, slots, span), bf16),
            pltpu.VMEM((batch, span), f32),
            pltpu.VMEM((n_ep, seq_rows, span), bf16),
            pltpu.VMEM((n_ep, seq_rows, span), bf16),
            dma((10,)),
            dma((seq_rows // 8,)),
            dma((9,)),
            dma, dma,
            dma, dma((n_ep,)),
            dma, dma((n_sets,)),
            dma((n_sets,)), dma((n_sets,)),
            dma, dma,
        ],
        compiler_params=pltpu.CompilerParams(
            collective_id=0, has_side_effects=True, vmem_limit_bytes=VMEM_BYTES),
        name="whole_layer",
    )(tokens, attn_gain.reshape(1, width), query_gain.reshape(1, -1), key_gain.reshape(1, -1),
      w_forget.reshape(1, width), forget_bias.reshape(1, 1), lengths.reshape(1, seq_rows),
      ffn_gain.reshape(1, width), expert_ids.T, route_weight.T, shared_gate.reshape(width // 128, 128),
      w_query, w_key.T, w_value.T, cache_cum, cache_pairs, w_output,
      w_exp_gate, w_exp_up, w_exp_down,
      w_dense_gate, w_dense_up, w_dense_down)


def shards(
    tokens,
    attn_gain,
    w_query,
    w_key,
    w_value,
    w_forget,
    forget_bias,
    query_gain,
    key_gain,
    cache_pairs,
    cache_cum,
    lengths,
    w_output,
    ffn_gain,
    expert_ids,
    route_weight,
    w_exp_gate,
    w_exp_up,
    w_exp_down,
    shared_gate,
    w_dense_gate,
    w_dense_up,
    w_dense_down,
):
    return layer_call(
        tokens, attn_gain, w_query, w_key, w_value, w_forget, forget_bias, query_gain, key_gain,
        cache_pairs, cache_cum, lengths, w_output, ffn_gain, expert_ids, route_weight, shared_gate,
        w_exp_gate, w_exp_up, w_exp_down, w_dense_gate, w_dense_up, w_dense_down,
    )


def solution(mesh):
    in_specs = (
        P("ep", None),
        P(),
        P(None, "tp"),
        P(None, "tp"),
        P(None, "tp"),
        P(None, "tp"),
        P("tp"),
        P(),
        P(),
        P("ep", "tp", None, None),
        P("ep", "tp", None),
        P("ep"),
        P("tp", None),
        P(),
        P(),
        P(),
        P("ep", None, "tp"),
        P("ep", None, "tp"),
        P("ep", "tp", None),
        P(),
        P("ep", None),
        P("ep", None),
        P("ep", "tp"),
    )
    out_specs = P("ep", "tp")
    return jax.shard_map(shards, mesh=mesh, in_specs=in_specs, out_specs=out_specs, check_vma=False)
```

```python
import functools

import jax
import jax.numpy as jnp
from jax import lax
from jax.experimental import pallas as pl
from jax.experimental.pallas import tpu as pltpu
from jax.sharding import PartitionSpec as P

EPSILON = 1e-06
MESH = pl.DeviceIdType.MESH
VMEM_BYTES = 56 * 1024 * 1024


def block_sets(n_ep):
    if n_ep == 8:
        return [[0], [1, 2, 3], [4, 5, 6, 7]]
    return [list(range(n_ep))]


def whole_layer(
    n_ep, n_tp, cap,
    tokens_hbm, attn_gain_hbm, query_gain_hbm, key_gain_hbm, forget_hbm, bias_hbm, length_hbm,
    gain_hbm, ids_hbm, route_hbm, shared_hbm,
    wq_hbm, wk_hbm, wv_hbm, cum_hbm, cache_hbm, wo_hbm,
    wg_hbm, wu_hbm, wd_hbm, dg_hbm, du_hbm, dd_hbm,
    out_ref,
    tokens_ref, attn_gain_ref, query_gain_ref, key_gain_ref, forget_ref, bias_ref, length_ref,
    gain_ref, ids_ref, route_ref, shared_ref,
    wq, wkv, cum, cache, wo_ref, mixed,
    wgu, wd, dgu, dd,
    part_out, part_in, gathered, rows_f, pick_ref, place_ref, weight_ref, mix_ref, exp_out, exp_in, total, sum_out, sum_in,
    small_sem, attn_sem, load_sem, part_send, part_recv, ring_send, ring_recv, fan_send, fan_recv,
    exp_send, exp_recv, sum_send, sum_recv,
):
    me = lax.axis_index("ep")
    col = lax.axis_index("tp")
    seq_rows, width = tokens_ref.shape
    span = width // n_tp
    slots = n_ep * cap
    batch = n_ep * seq_rows
    f32, bf16 = jnp.float32, jnp.bfloat16
    head = query_gain_ref.shape[1]
    heads = wq.shape[1] // head
    lanes = 2 * head
    eight = 8
    bunch = eight
    small = [
        pltpu.make_async_copy(src, dst, small_sem.at[i])
        for i, (src, dst) in enumerate((
            (tokens_hbm, tokens_ref), (attn_gain_hbm, attn_gain_ref), (wq_hbm, wq),
            (wk_hbm, wkv.at[pl.ds(0, head)]),
            (forget_hbm, forget_ref), (bias_hbm, bias_ref), (length_hbm, length_ref),
            (query_gain_hbm, query_gain_ref), (key_gain_hbm, key_gain_ref), (cum_hbm.at[:, 0], cum)))
    ]
    small.insert(4, pltpu.make_async_copy(wv_hbm, wkv.at[pl.ds(head, head)], small_sem.at[3]))
    both = pltpu.make_async_copy(wkv, wkv, small_sem.at[3])
    caches = [
        pltpu.make_async_copy(cache_hbm.at[pl.ds(b, bunch), 0], cache.at[pl.ds(b, bunch)], attn_sem.at[b // bunch])
        for b in range(0, seq_rows, bunch)
    ]
    later = [
        pltpu.make_async_copy(src, dst, load_sem.at[i])
        for i, (src, dst) in enumerate((
            (wo_hbm, wo_ref), (gain_hbm, gain_ref), (ids_hbm, ids_ref), (route_hbm, route_ref),
            (shared_hbm, shared_ref), (wg_hbm, wgu.at[pl.ds(0, 1)]), (wd_hbm.at[0], wd),
            (dg_hbm, dgu.at[0]), (dd_hbm, dd)))
    ]
    later.insert(6, pltpu.make_async_copy(wu_hbm, wgu.at[pl.ds(1, 1)], load_sem.at[5]))
    later.insert(9, pltpu.make_async_copy(du_hbm, dgu.at[1], load_sem.at[7]))
    held = [pltpu.make_async_copy(wgu, wgu, load_sem.at[5]), later[7], pltpu.make_async_copy(dgu, dgu, load_sem.at[7]), later[10]]
    for load in small + caches + later[:5]:
        load.start()

    barrier = pltpu.get_barrier_semaphore()
    for k in range(1, n_ep):
        pl.semaphore_signal(barrier, inc=1, device_id={"ep": lax.rem(me + k, n_ep)}, device_id_type=MESH)
    for d in range(1, n_tp):
        pl.semaphore_signal(barrier, inc=1, device_id={"tp": lax.rem(col + d, n_tp)}, device_id_type=MESH)

    def columns(d):
        return pl.ds(pl.multiple_of(lax.rem(col + d, n_tp) * span, span), span)

    def to_tp(src, dst, send, recv, d):
        return pltpu.make_async_remote_copy(
            src_ref=src, dst_ref=dst, send_sem=send, recv_sem=recv,
            device_id={"tp": lax.rem(col + d, n_tp)}, device_id_type=MESH)

    def to_ep(src, dst, send, recv, peer):
        return pltpu.make_async_remote_copy(
            src_ref=src, dst_ref=dst, send_sem=send, recv_sem=recv,
            device_id={"ep": peer}, device_id_type=MESH)

    if n_ep == 8:
        deep, side = me // 2, lax.rem(me, 2)
        low = (deep < 2).astype(jnp.int32)
        inner = low * deep + (1 - low) * (3 - deep)
        line = [inner, 1 - inner, 2, 3]
        line = [low * at + (1 - low) * (3 - at) for at in line]
        away = [line[k // 2] * 2 + (side if k % 2 == 0 else 1 - side) for k in range(n_ep - 1, 0, -1)]
    else:
        away = [lax.rem(me + k, n_ep) for k in range(1, n_ep)]
    rising = [k + (me <= k).astype(jnp.int32) for k in range(n_ep - 1)]
    sets = block_sets(n_ep)

    contract = (((1,), (1,)), ((), ()))

    def iota(shape, axis):
        return lax.broadcasted_iota(jnp.int32, shape, axis).astype(f32)

    def group_of(values, size):
        return jnp.floor((values + 0.5) * (1.0 / size))

    def rms(values, gain):
        return values * lax.rsqrt(jnp.mean(values * values, axis=1, keepdims=True) + EPSILON) * gain

    def rounded(values):
        return values.astype(bf16).astype(f32)

    def half_turn(values):
        return pltpu.roll(values, head, 1)

    left = lax.broadcasted_iota(jnp.int32, (seq_rows, lanes), 1) < head
    small[0].wait()
    small[1].wait()
    token_f = tokens_ref[...].astype(f32)
    normed_one = rms(token_f, attn_gain_ref[...]).astype(bf16)
    small[2].wait()
    query_raw = jnp.dot(normed_one, wq[...], preferred_element_type=f32)
    for load in [both] + small[5:10]:
        load.wait()
    pair_raw = lax.dot_general(normed_one, wkv[...], contract, preferred_element_type=f32)
    gate_in = jnp.sum(normed_one.astype(f32) * forget_ref[...].astype(f32), axis=1, keepdims=True) + bias_ref[...]
    log_gate = jnp.minimum(gate_in, 0.0) - jnp.log(1.0 + jnp.exp(-jnp.abs(gate_in)))
    eye = iota((seq_rows, seq_rows), 0) == iota((seq_rows, seq_rows), 1)
    lengths = jnp.sum(jnp.where(eye, jnp.broadcast_to(length_ref[...].astype(f32), (seq_rows, seq_rows)), 0.0), axis=1, keepdims=True)

    def half_scales(values):
        squares = values * values
        first = jnp.sum(jnp.where(left, squares, 0.0), axis=1, keepdims=True)
        second = jnp.sum(jnp.where(left, 0.0, squares), axis=1, keepdims=True)
        return lax.rsqrt(first / head + EPSILON), lax.rsqrt(second / head + EPSILON)

    gain_twice = jnp.concatenate([query_gain_ref[...]] * 2, axis=1)
    queries = []
    for a in range(heads // 2):
        raw = query_raw[:, lanes * a:lanes * (a + 1)]
        first, second = half_scales(raw)
        query = rounded(raw * jnp.where(left, first, second) * gain_twice)
        turned = half_turn(query)
        queries += [jnp.where(left, query, turned), jnp.where(left, turned, query)]
    key_scale, _ = half_scales(pair_raw)
    key_gain = jnp.concatenate([key_gain_ref[...]] * 2, axis=1)
    key = jnp.where(left, rounded(pair_raw * key_scale * key_gain), 0.0)
    value = rounded(pair_raw)
    value = jnp.where(left, half_turn(value), value)
    multiplier = head ** (-0.5)
    own_scores = [jnp.sum(query * key, axis=1, keepdims=True) * multiplier for query in queries]
    scaled = [query * multiplier for query in queries]
    small[10].wait()
    position = iota(cum.shape, 1)
    now = jnp.sum(jnp.where(position == lengths - 1.0, cum[...], 0.0), axis=1, keepdims=True) + log_gate
    cum[...] = jnp.where(position < lengths, now - cum[...], -1e30)

    row = lax.broadcasted_iota(jnp.int32, (eight, lanes), 0)
    left_eight = lax.broadcasted_iota(jnp.int32, (eight, lanes), 1) < head
    key_at = [row == jnp.where(left_eight, 2 * p, 2 * p + 1) for p in range(eight // 2)]
    value_at = [row == jnp.where(left_eight, 2 * p + 1, 2 * p) for p in range(eight // 2)]

    def score_of(i):
        lines = slice(i * eight, (i + 1) * eight)
        lhs = jnp.concatenate([
            jnp.concatenate([jnp.where(key_at[p], query[lines], 0.0) for query in scaled], axis=0)
            for p in range(eight // 2)], axis=1).astype(bf16)
        keys = jnp.concatenate([cache[i * eight + b, :, 0:head] for b in range(eight)], axis=1)
        return lax.dot_general(lhs, keys, contract, preferred_element_type=f32)

    def attend(i, score):
        lines = slice(i * eight, (i + 1) * eight)
        score = score + jnp.concatenate([cum[lines, :]] * heads, axis=0)
        own = jnp.concatenate([values[lines] for values in own_scores], axis=0)
        peak = jnp.maximum(jnp.max(score, axis=1, keepdims=True), own)
        past = jnp.exp(score - peak)
        own = jnp.exp(own - peak)
        inverse = 1.0 / (jnp.sum(past, axis=1, keepdims=True) + own)
        prob = (past * inverse).astype(bf16)
        own = rounded(own * inverse)
        return prob, own

    def gather_values(i, prob, own):
        lines = slice(i * eight, (i + 1) * eight)
        values = jnp.concatenate([cache[i * eight + (b ^ 1), :, head:2 * head] for b in range(eight)], axis=1)
        wide = jnp.dot(prob, values, preferred_element_type=f32)
        mixes = []
        for h in range(heads):
            here = slice(h * eight, (h + 1) * eight)
            mix = sum(jnp.where(value_at[p], wide[here, lanes * p:lanes * (p + 1)], 0.0) for p in range(eight // 2))
            mixes.append(mix + half_turn(mix) + own[here] * value[lines])
        for a in range(heads // 2):
            mixed[lines, lanes * a:lanes * (a + 1)] = jnp.where(left_eight, mixes[2 * a], mixes[2 * a + 1])

    count = seq_rows // eight
    score, prob = {}, {}
    for i in range(count):
        for load in caches[i * eight // bunch:(i + 1) * eight // bunch]:
            load.wait()
        if i > 0:
            prob[i - 1] = attend(i - 1, score[i - 1])
        score[i] = score_of(i)
    prob[count - 1] = attend(count - 1, score[count - 1])
    for i in range(count):
        gather_values(i, *prob[i])
    for load in later[5:]:
        load.start()
    head_mix = mixed[...].astype(bf16)
    later[0].wait()

    partial = jnp.dot(head_mix, wo_ref[...], preferred_element_type=f32).astype(bf16)
    for j in range(n_tp):
        part_out[j] = partial[:, j * span:(j + 1) * span]
    pl.semaphore_wait(barrier, n_ep + n_tp - 2)
    for d in sorted(range(1, n_tp), key=lambda d: d != 2):
        there = lax.rem(col + d, n_tp)
        to_tp(part_out.at[there], part_in.at[col], part_send, part_recv, d).start()
    some = pl.ds(0, n_tp - 1)
    parts = to_tp(part_out.at[some], part_in.at[some], part_send, part_recv, 1)
    token_block = tokens_ref[:, columns(0)].astype(f32)
    part_in[col] = part_out[col]
    parts.wait_recv()
    attn = part_in[0].astype(f32)
    for j in range(1, n_tp):
        attn = attn + part_in[j].astype(f32)
    residual = (token_block + attn).astype(bf16)
    gathered[col, me] = residual

    for peer in away:
        to_ep(gathered.at[col, me], gathered.at[col, me], ring_send, ring_recv.at[me], peer).start()
    if n_tp == 4:
        across = lax.rem(col + 2, 4)
        others = [across, across + 1 - 2 * lax.rem(col, 2), col + 1 - 2 * lax.rem(col, 2)]
    else:
        others = [lax.rem(col + d, n_tp) for d in range(1, n_tp)]

    def fan(slot):
        for other in others:
            pltpu.make_async_remote_copy(
                src_ref=gathered.at[col, slot], dst_ref=gathered.at[col, slot],
                send_sem=fan_send, recv_sem=fan_recv.at[set_of(slot)],
                device_id={"tp": other}, device_id_type=MESH).start()

    def set_of(slot):
        return sum((slot >= chosen[0]).astype(jnp.int32) for chosen in sets) - 1

    def spread(n):
        group = gathered.at[pl.ds(0, n_tp - 1), pl.ds(sets[n][0], len(sets[n]))]
        return pltpu.make_async_remote_copy(
            src_ref=group, dst_ref=group, send_sem=fan_send, recv_sem=fan_recv.at[n],
            device_id={"tp": others[0]}, device_id_type=MESH)

    fan(me)
    for load in later[1:5]:
        load.wait()
    def token_lines(chosen):
        return slice(chosen[0] * seq_rows, (chosen[-1] + 1) * seq_rows)

    def slot_lines(chosen):
        return slice(chosen[0] * cap, (chosen[-1] + 1) * cap)

    expert = me
    hit = jnp.zeros((1, batch), f32)
    weight_row = jnp.zeros((1, batch), f32)
    for k in range(ids_ref.shape[0]):
        same = ids_ref[k:k + 1, :] == expert
        hit = hit + jnp.where(same, 1.0, 0.0)
        weight_row = weight_row + jnp.where(same, route_ref[k:k + 1, :], 0.0)
    row_at = iota((batch, batch), 0)
    col_at = iota((batch, batch), 1)
    hits = jnp.broadcast_to(hit, (8, batch)).astype(bf16)
    hit = hits[0:1].astype(f32)
    before = (row_at <= col_at) & (row_at >= group_of(col_at, seq_rows) * seq_rows)
    rank = jnp.dot(hits, before.astype(f32).astype(bf16), preferred_element_type=f32)[0:1]
    slot_of = jnp.where((hit > 0.5) & (rank < cap + 0.5), group_of(iota((1, batch), 1), seq_rows) * cap + rank - 1.0, -1.0)
    for n, chosen in enumerate(sets):
        lines, places = token_lines(chosen), slot_lines(chosen)
        here = slot_of[:, lines]
        size = len(chosen) * cap, len(chosen) * seq_rows
        pick = jnp.where(iota(size, 0) + chosen[0] * cap == here, 1.0, 0.0)
        pick_ref[n, 0:size[0], 0:size[1]] = pick.astype(bf16)
        place_ref[n, 0:size[1], 0:size[0]] = pick.T.astype(bf16)
        weight_ref[lines, :] = jnp.sum((pick * weight_row[:, lines]).T, axis=1, keepdims=True)
    shared_tiles = shared_ref[...].astype(f32)
    shared = jnp.concatenate([shared_tiles[i:i + 1] for i in range(width // 128)], axis=1)

    def lines_of(slot):
        return slice(slot * seq_rows, (slot + 1) * seq_rows)

    def normalize(k):
        blocks = [gathered[t, k].astype(f32) for t in range(n_tp)]
        squares = sum(jnp.sum(b * b, axis=1, keepdims=True) for b in blocks)
        scale = lax.rsqrt(squares / width + EPSILON)
        for t in range(n_tp):
            rows_f[lines_of(k), t * span:(t + 1) * span] = (
                blocks[t] * scale * gain_ref[:, t * span:(t + 1) * span])

    def prepare(n):
        chosen = sets[n]
        for k in chosen:
            normalize(k)
        rows = rows_f[token_lines(chosen), :].astype(bf16)
        mix = jnp.sum(rows.astype(f32) * shared, axis=1, keepdims=True)
        mix_ref[token_lines(chosen), :] = 1.0 / (1.0 + jnp.exp(-mix))
        pick = pick_ref[n, 0:len(chosen) * cap, 0:len(chosen) * seq_rows]
        return jnp.dot(pick, rows, preferred_element_type=f32).astype(bf16)

    def hidden_of(picked):
        gate = jnp.dot(picked, wgu[0], preferred_element_type=f32)
        up = jnp.dot(picked, wgu[1], preferred_element_type=f32)
        return (gate / (1.0 + jnp.exp(-gate)) * up).astype(bf16)

    def down_of(hidden):
        return jnp.dot(hidden, wd[...], preferred_element_type=f32).astype(bf16)

    def send_moves(n, down):
        chosen = sets[n]
        places = slot_lines(chosen)
        for j in range(n_tp):
            exp_out[j, places, :] = down[:, j * span:(j + 1) * span]
        part = pl.ds(chosen[0] * cap, len(chosen) * cap)
        for d in sorted(range(1, n_tp), key=lambda d: d != 2):
            there = lax.rem(col + d, n_tp)
            to_tp(exp_out.at[there, part], exp_in.at[col, part], exp_send.at[n], exp_recv.at[n], d).start()
        exp_in[col, places, :] = exp_out[col, places, :]

    def moves(n):
        there = exp_in.at[pl.ds(0, n_tp - 1), pl.ds(sets[n][0] * cap, len(sets[n]) * cap)]
        return to_tp(there, there, exp_send.at[n], exp_recv.at[n], 1)

    def dense(rows):
        rows = rows.astype(bf16)
        gate = lax.dot_general(rows, dgu[0], contract, preferred_element_type=f32)
        up = lax.dot_general(rows, dgu[1], contract, preferred_element_type=f32)
        hidden = (gate / (1.0 + jnp.exp(-gate)) * up).astype(bf16)
        return jnp.dot(hidden, dd[...], preferred_element_type=f32)

    def finish(n, chosen):
        moves(n).wait_recv()
        places, lines = slot_lines(chosen), token_lines(chosen)
        rows = exp_in[0, places, :].astype(f32)
        for j in range(1, n_tp):
            rows = rows + exp_in[j, places, :].astype(f32)
        place = place_ref[n, 0:len(chosen) * seq_rows, 0:len(chosen) * cap]
        placed = jnp.dot(place, rows.astype(bf16), preferred_element_type=f32) * weight_ref[lines, :]
        total[lines, :] = total[lines, :] + placed
        for slot in chosen:
            sum_out[slot] = total[lines_of(slot), :].astype(bf16)
        for slot in (chosen if 2 * n < len(sets) else reversed(chosen)):
            @pl.when(slot != me)
            def _():
                to_ep(sum_out.at[slot], sum_in.at[me], sum_send, sum_recv, slot).start()

    for slot in rising:
        to_ep(gathered.at[col, slot], gathered.at[col, slot], ring_send, ring_recv.at[slot], slot).wait_recv()
        fan(slot)
    for load in held:
        load.wait()
    spread(0).wait_recv()
    picked = prepare(0)
    for n in range(len(sets)):
        hidden = hidden_of(picked)
        if n + 1 < len(sets) and n > 0:
            spread(n + 1).wait_recv()
        down = down_of(hidden)
        if n + 1 < len(sets) and n > 0:
            picked = prepare(n + 1)
        send_moves(n, down)
        if n + 1 < len(sets) and n == 0:
            spread(n + 1).wait_recv()
            picked = prepare(n + 1)
    step = seq_rows * 8 if n_ep % 8 == 0 else batch
    if step == batch:
        total[...] = mix_ref[...] * dense(rows_f[...])
    else:
        @pl.loop(0, batch // step)
        def _(i):
            at = pl.multiple_of(i * step, step)
            total[pl.ds(at, step), :] = mix_ref[pl.ds(at, step), :] * dense(rows_f[pl.ds(at, step), :])
    for n, chosen in enumerate(sets):
        finish(n, chosen)
    most = pl.ds(0, n_ep - 1)
    result = residual.astype(f32) + total[pl.ds(pl.multiple_of(me * seq_rows, 8), seq_rows), :]
    sums = to_ep(sum_in.at[most], sum_in.at[most], sum_send, sum_recv, away[0])
    sums.wait_recv()
    sum_in[me] = jnp.zeros_like(sum_in[me])
    for slot in range(n_ep):
        result = result + sum_in[slot].astype(f32)
    out_ref[...] = result.astype(bf16)
    parts.wait_send()
    to_ep(gathered.at[0, most], gathered.at[0, most], ring_send, ring_recv.at[0], away[0]).wait_send()
    for n in range(len(sets)):
        spread(n).wait_send()
    for n in range(len(sets)):
        moves(n).wait_send()
    sums.wait_send()


def layer_call(tokens, attn_gain, w_query, w_key, w_value, w_forget, forget_bias, query_gain, key_gain,
              cache_pairs, cache_cum, lengths, w_output, ffn_gain, expert_ids, route_weight, shared_gate,
              w_exp_gate, w_exp_up, w_exp_down, w_dense_gate, w_dense_up, w_dense_down):
    n_ep, n_tp = lax.axis_size("ep"), lax.axis_size("tp")
    seq_rows, width = tokens.shape
    cap = max(2, min(seq_rows, 128 // n_ep))
    sets = block_sets(n_ep)
    n_sets, most = len(sets), max(len(chosen) for chosen in sets)
    span = width // n_tp
    slots, batch = n_ep * cap, n_ep * seq_rows
    bf16, f32 = jnp.bfloat16, jnp.float32
    vmem = pl.BlockSpec(memory_space=pltpu.VMEM)
    hbm = pl.BlockSpec(memory_space=pltpu.HBM)
    dma = pltpu.SemaphoreType.DMA
    return pl.pallas_call(
        functools.partial(whole_layer, n_ep, n_tp, cap),
        out_shape=pltpu.VMEM((seq_rows, span), bf16),
        in_specs=[hbm] * 23,
        out_specs=vmem,
        scratch_shapes=[
            pltpu.VMEM(tokens.shape, bf16),
            pltpu.VMEM((1, width), f32),
            pltpu.VMEM((1, query_gain.shape[0]), f32),
            pltpu.VMEM((1, key_gain.shape[0]), f32),
            pltpu.VMEM((1, width), bf16),
            pltpu.VMEM((1, 1), f32),
            pltpu.VMEM((1, seq_rows), jnp.int32),
            pltpu.VMEM((1, width), f32),
            pltpu.VMEM(expert_ids.shape[::-1], jnp.int32),
            pltpu.VMEM(route_weight.shape[::-1], f32),
            pltpu.VMEM((width // 128, 128), bf16),
            pltpu.VMEM(w_query.shape, bf16),
            pltpu.VMEM((2 * w_key.shape[1], width), bf16),
            pltpu.VMEM((seq_rows, cache_cum.shape[2]), f32),
            pltpu.VMEM((seq_rows,) + cache_pairs.shape[2:], bf16),
            pltpu.VMEM(w_output.shape, bf16),
            pltpu.VMEM((seq_rows, w_query.shape[1]), f32),
            pltpu.VMEM((2,) + w_exp_gate.shape[1:], bf16),
            pltpu.VMEM(w_exp_down.shape[1:], bf16),
            pltpu.VMEM((2,) + w_dense_gate.shape, bf16),
            pltpu.VMEM(w_dense_down.shape, bf16),
            pltpu.VMEM((n_tp, seq_rows, span), bf16),
            pltpu.VMEM((n_tp, seq_rows, span), bf16),
            pltpu.VMEM((n_tp, n_ep, seq_rows, span), bf16),
            pltpu.VMEM((batch, width), f32),
            pltpu.VMEM((n_sets, most * cap, most * seq_rows), bf16),
            pltpu.VMEM((n_sets, most * seq_rows, most * cap), bf16),
            pltpu.VMEM((batch, 1), f32),
            pltpu.VMEM((batch, 1), f32),
            pltpu.VMEM((n_tp, slots, span), bf16),
            pltpu.VMEM((n_tp, slots, span), bf16),
            pltpu.VMEM((batch, span), f32),
            pltpu.VMEM((n_ep, seq_rows, span), bf16),
            pltpu.VMEM((n_ep, seq_rows, span), bf16),
            dma((10,)),
            dma((seq_rows // 8,)),
            dma((9,)),
            dma, dma,
            dma, dma((n_ep,)),
            dma, dma((n_sets,)),
            dma((n_sets,)), dma((n_sets,)),
            dma, dma,
        ],
        compiler_params=pltpu.CompilerParams(
            collective_id=0, has_side_effects=True, vmem_limit_bytes=VMEM_BYTES),
        name="whole_layer",
    )(tokens, attn_gain.reshape(1, width), query_gain.reshape(1, -1), key_gain.reshape(1, -1),
      w_forget.reshape(1, width), forget_bias.reshape(1, 1), lengths.reshape(1, seq_rows),
      ffn_gain.reshape(1, width), expert_ids.T, route_weight.T, shared_gate.reshape(width // 128, 128),
      w_query, w_key.T, w_value.T, cache_cum, cache_pairs, w_output,
      w_exp_gate, w_exp_up, w_exp_down,
      w_dense_gate, w_dense_up, w_dense_down)


def shards(
    tokens,
    attn_gain,
    w_query,
    w_key,
    w_value,
    w_forget,
    forget_bias,
    query_gain,
    key_gain,
    cache_pairs,
    cache_cum,
    lengths,
    w_output,
    ffn_gain,
    expert_ids,
    route_weight,
    w_exp_gate,
    w_exp_up,
    w_exp_down,
    shared_gate,
    w_dense_gate,
    w_dense_up,
    w_dense_down,
):
    return layer_call(
        tokens, attn_gain, w_query, w_key, w_value, w_forget, forget_bias, query_gain, key_gain,
        cache_pairs, cache_cum, lengths, w_output, ffn_gain, expert_ids, route_weight, shared_gate,
        w_exp_gate, w_exp_up, w_exp_down, w_dense_gate, w_dense_up, w_dense_down,
    )


def solution(mesh):
    in_specs = (
        P("ep", None),
        P(),
        P(None, "tp"),
        P(None, "tp"),
        P(None, "tp"),
        P(None, "tp"),
        P("tp"),
        P(),
        P(),
        P("ep", "tp", None, None),
        P("ep", "tp", None),
        P("ep"),
        P("tp", None),
        P(),
        P(),
        P(),
        P("ep", None, "tp"),
        P("ep", None, "tp"),
        P("ep", "tp", None),
        P(),
        P("ep", None),
        P("ep", None),
        P("ep", "tp"),
    )
    out_specs = P("ep", "tp")
    return jax.shard_map(shards, mesh=mesh, in_specs=in_specs, out_specs=out_specs, check_vma=False)
```
